128 devices in a mesh: sp: 64 (over z, y, x), tp: 2 (over core).
Axes of the slice: x: 4, y: 4, z: 4, core: 2. Of those that a mesh axis runs over, the one named last changes fastest.
Arguments:
- stream_rows: bfloat16 [12288, 2048], P('sp'), may hold values from -6 to 6
- out_cotangent: bfloat16 [12288, 2048], P('sp'), may hold values from -16 to 16
- expert_ids: int32 [12288, 2], P('sp'), may hold values from 0 to 63, all different within a row; in each aligned block of 192 rows (0 to 191, 192 to 383, ...) at most 9 rows name the same one
- route_weights: float32 [12288, 2], P('sp'), may hold values from 0.05 to 1
- gate_weight: bfloat16 [64, 2048, 1536], P('sp', None, 'tp'), may hold values from -0.125 to 0.125
- up_weight: bfloat16 [64, 2048, 1536], P('sp', None, 'tp'), may hold values from -0.125 to 0.125
- down_weight: bfloat16 [64, 1536, 2048], P('sp', 'tp'), may hold values from -0.15625 to 0.15625
- proj_weight: bfloat16 [1024, 2048], P('tp'), may hold values from -0.1875 to 0.1875
- gate_input: bfloat16 [12288, 1024], P('sp', 'tp'), may hold values from -6 to 6
- scan_out: bfloat16 [12288, 1024], P('sp', 'tp'), may hold values from -6 to 6
- values: bfloat16 [12288, 1024], P('sp', 'tp'), may hold values from -6 to 6
- in_map: bfloat16 [12288, 512], P('sp', 'tp'), may hold values from -2 to 2
- out_map: bfloat16 [12288, 512], P('sp', 'tp'), may hold values from -2 to 2
- log_decay: float32 [12288, 16], P('sp', 'tp'), may hold values from -2 to 0, as said below
Outputs:
- stream_grad: bfloat16 [12288, 2048], P('sp', 'tp')
- proj_grad: float32 [2048, 1024], P('sp', 'tp')
- value_grad: bfloat16 [12288, 1024], P('sp', 'tp')
- in_map_grad: bfloat16 [12288, 512], P('sp', 'tp')
- out_map_grad: bfloat16 [12288, 512], P('sp', 'tp')
- gate_input_grad: bfloat16 [12288, 1024], P('sp', 'tp')
- gate_weight_grad: bfloat16 [64, 2048, 1536], P('sp', None, 'tp')
- up_weight_grad: bfloat16 [64, 2048, 1536], P('sp', None, 'tp')
- down_matrix_gradient: bfloat16 [64, 1536, 2048], P('sp', 'tp')
The draws below stay inside these ranges and needn't reach their ends.
Inputs may be any that keep to these rules, and one draw needn't show every extreme that they name: `expert_ids`: the 2 experts of a token differ; among the tokens of one index of sp each expert is named at most 9 times, and exactly 9 times in some. `log_decay`: every entry is negative.
All inputs are finite; a program needn't handle non-finite values.
Results may differ from the reference program's by a relative error of at most 0.007.
Values may be sent and summed in bfloat16 or wider, within the bound.
No kernel may reach another device: no remote copies, remote signals or barrier semaphores. Data moves between devices by JAX's collectives and lax.ppermute only.
A program may use at most 192 MiB of HBM per device.

```python
import math
import jax
import jax.numpy as jnp
import numpy as np
from jax import lax

D = 2048
HEADS = 16
HEAD_DIM = 64
GROUPS = 4
STATE = 128
FF = 1536
TOP_K = 2
TOK_DEV = 192
SEQUENCE_TOKENS = 12288
EXPERTS = 64
CAP = 9
DS = 1024
N_SP = 64
N_TP = 2


def draw_log_decay(key, part):
    random_subkeys = jax.random.split(key, 6)
    slow_heads = jax.random.uniform(random_subkeys[0], (HEADS,)) < 0.5
    data_part = 0.5 * jnp.clip(jax.random.normal(random_subkeys[1], (SEQUENCE_TOKENS, HEADS)), -3.0, 3.0)
    slow_total = jax.random.uniform(random_subkeys[2], (HEADS,), minval=0.1, maxval=0.4)
    fast_span = jax.random.uniform(random_subkeys[3], (HEADS,), minval=30.0, maxval=100.0)
    base_rate = jnp.where(slow_heads, slow_total / SEQUENCE_TOKENS, 1.0 / fast_span)
    block_scale = jnp.exp(jax.random.uniform(random_subkeys[4], (SEQUENCE_TOKENS // TOK_DEV,), minval=-math.log(2.0), maxval=math.log(2.0)))
    stable_phase = -base_rate[None, :] * jnp.repeat(block_scale, TOK_DEV)[:, None] * jnp.exp(data_part)
    packet_position = jax.random.randint(random_subkeys[5], (2,), 0, SEQUENCE_TOKENS)
    packet_length = jnp.log(jax.random.uniform(jax.random.fold_in(random_subkeys[5], 7), (2,), minval=0.55, maxval=0.8))
    packet_increment = jnp.zeros((SEQUENCE_TOKENS,), jnp.float32).at[packet_position].add(packet_length)
    return (stable_phase + packet_increment[:, None]).astype(jnp.float32)


def raised(entries, key, source, target, shards_of, factor):
    owner, partner = [(jnp.arange(entries.shape[dim]) // (entries.shape[dim] // shards_of)).reshape([-1 if axis == dim else 1 for axis in range(entries.ndim)]) for dim in (source, target)]
    chosen = jax.random.permutation(key, shards_of)[partner]
    strong = (owner == chosen) | (owner == (partner + shards_of // 2) % shards_of)
    return jnp.where(strong, factor * entries, entries)


def level_of(key, dims, shards, smallest, top_value):
    level = 1.0
    for dim, blocks in shards:
        draws = jax.random.uniform(jax.random.fold_in(jax.random.fold_in(key, 6), dim), (blocks,), jnp.float32, smallest / len(shards), top_value / len(shards))
        level = level * jnp.repeat(jnp.exp(draws), dims[dim] // blocks).reshape((-1,) + (1,) * (len(dims) - 1 - dim))
    return level


def deal_out(own_key, own, number, rows, count, top, most, skew):
    sequence = jax.random.permutation(own_key, count)
    crowded, ordinary = load_shares(count, rows * top, most, skew, True), load_shares(count, rows * top, most, skew, False)
    places = jnp.arange(count)

    def named(sizes, turn):
        used = int((sizes > 0).sum())
        fixed = max(1, used // 4)
        moved = fixed + (places - fixed + turn * (used - fixed)) % max(1, count - fixed)
        return jnp.zeros((count,), jnp.int32).at[sequence[jnp.where(places < fixed, places, moved)]].set(jnp.asarray(sizes, jnp.int32))

    sizes = jnp.where(number % 4 == 0, named(crowded, number // 4), named(ordinary, number - number // 4 - 1))
    mixed = jax.random.permutation(jax.random.fold_in(own, 3), count)
    donor, taker = mixed[0:count // 2 * 2:2], mixed[1:count // 2 * 2:2]
    room = jnp.minimum(sizes[donor] - 1, most - sizes[taker]) // 2
    room = jnp.where((donor == sequence[0]) | (taker == sequence[0]) | (sizes[taker] == 0), 0, jnp.maximum(room, 0))
    moved = jax.random.randint(jax.random.fold_in(own, 4), (count // 2,), 0, 1 << 20) % (room + 1)
    sizes = sizes.at[donor].add(-moved).at[taker].add(moved)
    items = jnp.searchsorted(jnp.cumsum(sizes), jnp.arange(rows * top), side="right").astype(jnp.int32)
    table = items.reshape(top, rows).T
    table = table[jax.random.permutation(jax.random.fold_in(own, 1), rows)]
    turn = jax.random.randint(jax.random.fold_in(own, 2), (rows, 1), 0, top)
    return jnp.take_along_axis(table, (jnp.arange(top)[None, :] + turn) % top, axis=1)


def load_shares(number_of, total, reach, skew, full):
    portions = [(1 << 20) // math.isqrt(rank ** skew) + 1 for rank in range(1, number_of + 1)]
    largest = reach if full else min(reach, max(-(-total // number_of), total * portions[0] // sum(portions)))
    least = 1 if total - largest >= number_of - 1 else 0
    counts, surplus = [largest] + [least] * (number_of - 1), total - largest - least * (number_of - 1)
    while surplus > 0:
        candidates = [i for i in range(1, number_of) if counts[i] < largest] or [i for i in range(1, number_of) if counts[i] < reach]
        whole, remaining = sum([portions[i] for i in candidates]), surplus
        for i in candidates:
            more = min(reach - counts[i], max(1, remaining * portions[i] // whole), surplus)
            counts[i] = counts[i] + more
            surplus = surplus - more
    return np.array(counts)


def gaussian(own_key, shape, scale, limit, pieces=(), kind=jnp.bfloat16):
    values = jax.random.normal(own_key, shape, jnp.float32) * scale
    if len(pieces) > 0:
        values = level_of(own_key, shape, pieces, -0.22, 0.18) * values
    return jnp.clip(values, min=-limit, max=limit).astype(kind)


def noise_with(rng, extent, scale, most, pieces, heavy, kind=jnp.bfloat16):
    drawn = scale * jax.random.normal(rng, extent, jnp.float32)
    if pieces:
        drawn = drawn * level_of(rng, extent, pieces, -0.22, 0.18)
    return jnp.clip(raised(drawn, jax.random.fold_in(rng, 3), *heavy), -most, most).astype(kind)


def setup_inputs(seed: int = 0) -> dict:
    splits = jax.random.split(jax.random.key(seed), 15)
    stream_rows = gaussian(splits[0], (SEQUENCE_TOKENS, D), 1.0, 6.0, ((0, 64),))
    out_cotangent = noise_with(splits[1], (SEQUENCE_TOKENS, D), 1.0, 16.0, ((0, 64),), (0, 1, 64, 4.0))
    expert_ids_keys = jax.random.split(jax.random.fold_in(splits[2], 1), SEQUENCE_TOKENS // TOK_DEV)
    expert_ids_turns = jax.random.permutation(jax.random.fold_in(splits[2], 3), SEQUENCE_TOKENS // TOK_DEV)
    expert_ids = jax.vmap(lambda own, number: deal_out(jax.random.fold_in(splits[2], 2), own, number, TOK_DEV, EXPERTS, TOP_K, CAP, 2))(expert_ids_keys, expert_ids_turns).reshape((SEQUENCE_TOKENS, TOP_K))
    route_weights = jnp.clip(0.05 + 0.95 * jax.random.uniform(splits[3], (SEQUENCE_TOKENS, TOP_K), jnp.float32) ** level_of(splits[3], (SEQUENCE_TOKENS, TOP_K), ((0, 64),), -0.2, 0.2), 0.05, 1.0)
    gate_weight = gaussian(splits[4], (EXPERTS, D, FF), D ** -0.5, 0.125, ((0, 64), (2, 2)))
    up_weight = gaussian(splits[5], (EXPERTS, D, FF), D ** -0.5, 0.125, ((0, 64), (2, 2)))
    down_weight = gaussian(splits[6], (EXPERTS, FF, D), FF ** -0.5, 0.15625, ((0, 64), (1, 2)))
    proj_weight = gaussian(splits[7], (DS, D), DS ** -0.5, 0.1875, ((0, 2),))
    gate_input = gaussian(splits[8], (SEQUENCE_TOKENS, DS), 1.0, 6.0, ((0, 64), (1, 2)))
    scan_out = gaussian(splits[9], (SEQUENCE_TOKENS, DS), 1.0, 6.0, ((0, 64), (1, 2)))
    values = gaussian(splits[10], (SEQUENCE_TOKENS, DS), 1.0, 6.0, ((0, 64), (1, 2)))
    in_map = gaussian(splits[11], (SEQUENCE_TOKENS, GROUPS * STATE), 0.3, 2.0, ((0, 64), (1, 2)))
    out_map = gaussian(splits[12], (SEQUENCE_TOKENS, GROUPS * STATE), 0.3, 2.0, ((0, 64), (1, 2)))
    log_decay = draw_log_decay(jax.random.fold_in(splits[14], 71), 0)
    return dict(stream_rows=stream_rows, out_cotangent=out_cotangent, expert_ids=expert_ids, route_weights=route_weights, gate_weight=gate_weight, up_weight=up_weight, down_weight=down_weight, proj_weight=proj_weight, gate_input=gate_input, scan_out=scan_out, values=values, in_map=in_map, out_map=out_map, log_decay=log_decay)


exact_mode = lax.Precision.HIGHEST


def silu_slope(pre_act):
    squash = jax.nn.sigmoid(pre_act)
    return squash * (1.0 + pre_act * (1.0 - squash))


def chain_states(earlier, later):
    factor = later[0][:, :, None, None]
    return (earlier[0] * later[0], factor * earlier[1] + later[1], factor * earlier[2] + later[2])


def block_states(value_heads, grad_heads, in_keys, out_keys, cum_decay):
    block_total = cum_decay[-1]
    to_end = jnp.exp(block_total[None] - cum_decay)
    from_start = jnp.exp(cum_decay)
    end_x = jnp.einsum('tge,tgep,tgn->gepn', to_end, value_heads, in_keys, precision=exact_mode)
    end_g = jnp.einsum('tge,tgep,tgn->gepn', to_end, grad_heads, out_keys, precision=exact_mode)
    start_x = jnp.einsum('tge,tgep,tgn->gepn', from_start, value_heads, in_keys, precision=exact_mode)
    start_g = jnp.einsum('tge,tgep,tgn->gepn', from_start, grad_heads, out_keys, precision=exact_mode)
    return jnp.exp(block_total), end_x, end_g, start_x, start_g


def local_grads(value_heads, grad_heads, in_keys, out_keys, cum_decay, left_x, left_g, right_x, right_g):
    block_total = cum_decay[-1]
    from_start = jnp.exp(cum_decay)
    to_end = jnp.exp(block_total[None] - cum_decay)
    cum_heads = jnp.transpose(cum_decay, (1, 2, 0))
    kernel = jnp.exp(-jnp.abs(cum_heads[..., :, None] - cum_heads[..., None, :]))
    intersection = jnp.einsum('tgn,sgn->gts', out_keys, in_keys, precision=exact_mode)
    weighted = kernel * intersection[:, None]
    value_grad = jnp.einsum('gets,tgep->sgep', weighted, grad_heads, precision=exact_mode)
    value_grad = value_grad + jnp.einsum('sge,gepn,sgn->sgep', from_start, left_g, in_keys, precision=exact_mode)
    value_grad = value_grad + jnp.einsum('sge,gepn,sgn->sgep', to_end, right_g, in_keys, precision=exact_mode)
    pair_weights = kernel * jnp.einsum('tgep,sgep->gets', grad_heads, value_heads, precision=exact_mode)
    out_grad = jnp.einsum('gets,sgn->tgn', pair_weights, in_keys, precision=exact_mode)
    out_grad = out_grad + jnp.einsum('tge,gepn,tgep->tgn', from_start, left_x, grad_heads, precision=exact_mode)
    out_grad = out_grad + jnp.einsum('tge,gepn,tgep->tgn', to_end, right_x, grad_heads, precision=exact_mode)
    in_grad = jnp.einsum('gets,tgn->sgn', pair_weights, out_keys, precision=exact_mode)
    in_grad = in_grad + jnp.einsum('sge,gepn,sgep->sgn', from_start, left_g, value_heads, precision=exact_mode)
    in_grad = in_grad + jnp.einsum('sge,gepn,sgep->sgn', to_end, right_g, value_heads, precision=exact_mode)
    return value_grad, in_grad, out_grad


def expert_pass(row_data, cotangent, gate_w, up_w, down_w):
    gate_pre = jnp.dot(row_data, gate_w, preferred_element_type=jnp.float32)
    up_val = jnp.dot(row_data, up_w, preferred_element_type=jnp.float32)
    active = (jax.nn.silu(gate_pre) * up_val).astype(jnp.bfloat16)
    down_grad = jnp.dot(active.T, cotangent, preferred_element_type=jnp.float32).astype(jnp.bfloat16)
    act_grad = jnp.dot(cotangent, down_w.T, preferred_element_type=jnp.float32)
    up_grad = (act_grad * jax.nn.silu(gate_pre)).astype(jnp.bfloat16)
    pre_grad = (act_grad * up_val * silu_slope(gate_pre)).astype(jnp.bfloat16)
    gate_w_grad = jnp.dot(row_data.T, pre_grad, preferred_element_type=jnp.float32).astype(jnp.bfloat16)
    up_w_grad = jnp.dot(row_data.T, up_grad, preferred_element_type=jnp.float32).astype(jnp.bfloat16)
    part_w = gate_w.shape[1] // N_TP
    summed = jnp.zeros((row_data.shape[0], gate_w.shape[0]), jnp.float32)
    for part_index in range(N_TP):
        low = part_index * part_w
        partial_value = jnp.dot(pre_grad[:, low:low + part_w], gate_w[:, low:low + part_w].T, preferred_element_type=jnp.float32)
        partial_value = partial_value + jnp.dot(up_grad[:, low:low + part_w], up_w[:, low:low + part_w].T, preferred_element_type=jnp.float32)
        rounded = lax.optimization_barrier(partial_value.astype(jnp.bfloat16))
        summed = summed + rounded.astype(jnp.float32)
    return summed.astype(jnp.bfloat16), gate_w_grad, up_w_grad, down_grad


def reference(stream_rows, out_cotangent, expert_ids, route_weights, gate_weight, up_weight, down_weight,
              proj_weight, gate_input, scan_out, values, in_map, out_map, log_decay):
    top_count = expert_ids.shape[1]
    flat_ids = expert_ids.reshape(-1).astype(jnp.int32)
    onehot = (flat_ids[:, None] == jnp.arange(EXPERTS, dtype=jnp.int32)[None, :]).astype(jnp.int32)
    onehot = onehot.reshape(N_SP, top_count * TOK_DEV, EXPERTS)
    rank_in = jnp.sum((jnp.cumsum(onehot, axis=1) - 1) * onehot, axis=2).reshape(-1)
    sentinel = SEQUENCE_TOKENS * top_count
    source = jnp.arange(sentinel, dtype=jnp.int32) // (top_count * TOK_DEV)
    position = (source * CAP + rank_in).astype(jnp.int32)
    table = jnp.full((EXPERTS, N_SP * CAP), sentinel, jnp.int32)
    table = table.at[flat_ids, position].set(jnp.arange(sentinel, dtype=jnp.int32))
    scaled = (route_weights[:, :, None] * out_cotangent[:, None, :].astype(jnp.float32)).astype(jnp.bfloat16)
    cot_pad = jnp.concatenate([scaled.reshape(sentinel, D), jnp.zeros((1, D), jnp.bfloat16)], axis=0)
    rows_pad = jnp.concatenate([stream_rows, jnp.zeros((1, D), jnp.bfloat16)], axis=0)

    def one_expert(operands):
        route_row, gate_w, up_w, down_w = operands
        row_data = rows_pad[route_row // top_count]
        cotangent = cot_pad[route_row]
        return expert_pass(row_data, cotangent, gate_w, up_w, down_w)

    row_grads, gate_grads, up_grads, down_grads = lax.map(one_expert, (table, gate_weight, up_weight, down_weight))
    returned = row_grads.reshape(-1, D)[flat_ids * (N_SP * CAP) + position].reshape(SEQUENCE_TOKENS, top_count, D)
    stream_grad = (out_cotangent.astype(jnp.float32) + jnp.sum(returned.astype(jnp.float32), axis=1)).astype(jnp.bfloat16)

    gate_vals = gate_input.astype(jnp.float32)
    scan_vals = scan_out.astype(jnp.float32)
    mixed_grad = jnp.dot(stream_grad, proj_weight.T, preferred_element_type=jnp.float32)
    gated = (scan_vals * jax.nn.silu(gate_vals)).astype(jnp.bfloat16)
    proj_grad = jnp.dot(stream_grad.T, gated, preferred_element_type=jnp.float32)
    gate_grad = (mixed_grad * scan_vals * silu_slope(gate_vals)).astype(jnp.bfloat16)
    scan_grad = (mixed_grad * jax.nn.silu(gate_vals)).astype(jnp.bfloat16)

    per_group = HEADS // GROUPS
    blocks_n = SEQUENCE_TOKENS // TOK_DEV
    value_heads = values.astype(jnp.float32).reshape(blocks_n, TOK_DEV, GROUPS, per_group, HEAD_DIM)
    grad_heads = scan_grad.astype(jnp.float32).reshape(blocks_n, TOK_DEV, GROUPS, per_group, HEAD_DIM)
    in_keys = in_map.astype(jnp.float32).reshape(blocks_n, TOK_DEV, GROUPS, STATE)
    out_keys = out_map.astype(jnp.float32).reshape(blocks_n, TOK_DEV, GROUPS, STATE)
    cum_decay = jnp.cumsum(log_decay.reshape(blocks_n, TOK_DEV, GROUPS, per_group), axis=1)

    def state_block(operands):
        return block_states(*operands)

    decay_tot, end_x, end_g, start_x, start_g = lax.map(state_block, (value_heads, grad_heads, in_keys, out_keys, cum_decay))
    identity = (jnp.ones((GROUPS, per_group), jnp.float32),
                jnp.zeros((GROUPS, per_group, HEAD_DIM, STATE), jnp.float32),
                jnp.zeros((GROUPS, per_group, HEAD_DIM, STATE), jnp.float32))

    def carry_step(carry, item):
        return chain_states(carry, item), carry

    left_end, left_state = lax.scan(carry_step, identity, (decay_tot, end_x, end_g))
    right_end, right_state = lax.scan(carry_step, identity, (decay_tot, start_x, start_g), reverse=True)

    def grad_block(operands):
        return local_grads(*operands)

    value_grad, in_grad, out_grad = lax.map(grad_block, (value_heads, grad_heads, in_keys, out_keys, cum_decay,
                                                         left_state[1], left_state[2], right_state[1], right_state[2]))
    value_grad = value_grad.reshape(SEQUENCE_TOKENS, DS).astype(jnp.bfloat16)
    in_grad = in_grad.reshape(SEQUENCE_TOKENS, GROUPS * STATE).astype(jnp.bfloat16)
    out_grad = out_grad.reshape(SEQUENCE_TOKENS, GROUPS * STATE).astype(jnp.bfloat16)
    return (stream_grad, proj_grad, value_grad, in_grad, out_grad, gate_grad, gate_grads, up_grads, down_grads)
```

```python
import jax
import jax.numpy as jnp
from jax import lax
from jax.experimental import pallas as pl
from jax.experimental.pallas import tpu as pltpu
from jax.sharding import Mesh
from jax.sharding import PartitionSpec as P

SP = ("sp_0", "sp_1", "sp_2")
TOK = 192
WIDTH = 2048
HALF = 1024
EXPERTS = 64
MAIN = 512
SLOTS = 576
FF = 768
FF_STEP = 256
CHAN = 512
KEYS = 256
HEADS = 8
BLOCKS = 64

BF = jnp.bfloat16
F32 = jnp.float32
EXACT = lax.Precision.HIGHEST


def mm(a, b, dims, precision=None):
    return lax.dot_general(a, b, (dims, ((), ())), preferred_element_type=F32, precision=precision)


NN = ((1,), (0,))
NT = ((1,), (1,))
TN = ((0,), (0,))


def iota(shape, dim):
    return lax.broadcasted_iota(jnp.int32, shape, dim)


def ones_where(mask):
    return jnp.where(mask, 1.0, 0.0).astype(BF)


def call(body, name, out_shape, flops, **kw):
    vmem = kw.pop("vmem", 40 << 20)
    return pl.pallas_call(
        body,
        out_shape=out_shape,
        name=name,
        compiler_params=pltpu.CompilerParams(vmem_limit_bytes=vmem),
        cost_estimate=pl.CostEstimate(flops=flops, bytes_accessed=1 << 20, transcendentals=0),
        **kw,
    )


def shape(dims, dtype=BF):
    return jax.ShapeDtypeStruct(dims, dtype)


def slot_choices(ids):
    lane = iota((TOK, EXPERTS), 1)
    named = [ids[:, k : k + 1] == lane for k in range(2)]
    either = ones_where(named[0] | named[1])
    earlier = ones_where(iota((TOK, TOK), 1) < iota((TOK, TOK), 0))
    count = mm(earlier, either, NN)
    picks = []
    for k in range(2):
        rank = jnp.sum(jnp.where(named[k], count, 0.0), axis=1, keepdims=True).astype(jnp.int32)
        own = ids[:, k : k + 1]
        row = jnp.where(rank < 8, own * 8 + rank, MAIN + own)
        picks.append(row == iota((TOK, SLOTS), 1))
    return picks


def fold_last(rows):
    q = iota((MAIN, MAIN), 0)
    order = ones_where(iota((MAIN, MAIN), 1) == (q & 7) * EXPERTS + (q >> 3))
    stacked = jnp.concatenate([rows[:, 128 * j : 128 * j + 128] for j in range(8)], axis=0)
    return mm(order, stacked, NN).astype(BF)


def unfold_last(folded):
    c = iota((MAIN, MAIN), 0)
    order = ones_where(iota((MAIN, MAIN), 1) == (c & 63) * 8 + (c >> 6))
    stacked = mm(order, folded, NN).astype(BF)
    return [
        jnp.concatenate(
            [stacked[64 * j : 64 * j + 64, 128 * i : 128 * i + 128] for j in range(8)], axis=1
        )
        for i in range(folded.shape[1] // 128)
    ]


def pack_body(tp, ids, weights, rows, cot, out):
    first, second = slot_choices(ids[...])
    both = ones_where(first | second)
    row_slots = mm(both, rows[...], TN).astype(BF)
    full = cot[...].astype(F32)
    cot_slots = mm(ones_where(first), (weights[:, 0:1] * full).astype(BF), TN)
    cot_slots = cot_slots + mm(ones_where(second), (weights[:, 1:2] * full).astype(BF), TN)
    cot_slots = cot_slots.astype(BF)
    out[:, 0:HALF] = row_slots[:MAIN]
    out[:, HALF : 2 * HALF] = cot_slots[:MAIN]
    out[:, 2 * HALF : 2 * HALF + 128] = fold_last(row_slots[MAIN:])
    out[:, 2 * HALF + 128 :] = fold_last(cot_slots[MAIN:])


def whole(dims):
    return pl.BlockSpec(dims, lambda *_: (0,) * len(dims))


def pack(tp, ids, weights, rows, cot):
    spec = pltpu.PrefetchScalarGridSpec(
        num_scalar_prefetch=1,
        grid=(1,),
        in_specs=[
            whole((TOK, 2)),
            whole((TOK, 2)),
            pl.BlockSpec((TOK, HALF), lambda i, t: (0, t[0])),
            pl.BlockSpec((TOK, HALF), lambda i, t: (0, t[0])),
        ],
        out_specs=whole((MAIN, 2 * HALF + 256)),
    )
    return call(
        pack_body, "pack", shape((MAIN, 2 * HALF + 256)), 1_000_000_000, grid_spec=spec
    )(tp, ids, weights, rows, cot)


def decay_body(values, in_map, log_decay, payload, start_w, end_w, cum_out, cum_t_out):
    upto = jnp.where(iota((TOK, TOK), 1) <= iota((TOK, TOK), 0), 1.0, 0.0)
    cum = mm(upto, log_decay[...], NN, EXACT)
    cum_t = mm(log_decay[...], upto, ((0,), (1,)), EXACT)
    cum_out[...] = cum
    cum_t_out[...] = cum_t
    spread = jnp.where(iota((HEADS, CHAN), 1) // 64 == iota((HEADS, CHAN), 0), 1.0, 0.0)
    from_start = mm(jnp.exp(cum), spread, NN, EXACT)
    to_end = mm(jnp.exp(cum[TOK - 1 :, :] - cum), spread, NN, EXACT)
    start_w[...] = from_start
    end_w[...] = to_end
    val = values[...].astype(F32)
    block_states(payload, (to_end * val).astype(BF), (from_start * val).astype(BF), in_map)
    total = jnp.exp(cum_t[:, TOK - 1 :])
    total = jnp.concatenate(
        [jnp.broadcast_to(total[h : h + 1], (64, 128)) for h in range(HEADS)], axis=0
    )
    high = total.astype(BF)
    rest = total - high.astype(F32)
    mid = rest.astype(BF)
    low = (rest - mid.astype(F32)).astype(BF)
    part = iota((MAIN, 128), 0) & 7
    parts = jnp.where(part == 0, high.astype(F32), 0.0)
    parts = jnp.where(part == 1, mid.astype(F32), parts)
    parts = jnp.where(part == 2, low.astype(F32), parts)
    payload[:, 256:] = parts.astype(BF)


def block_states(payload, to_end, from_start, keys):
    for g in range(2):
        chan = slice(256 * g, 256 * g + 256)
        key = keys[:, 128 * g : 128 * g + 128]
        payload[chan, 0:128] = mm(to_end[:, chan], key, TN).astype(BF)
        payload[chan, 128:256] = mm(from_start[:, chan], key, TN).astype(BF)


def decay(values, in_map, log_decay):
    return call(
        decay_body,
        "decay",
        (
            shape((MAIN, 384)),
            shape((TOK, CHAN), F32),
            shape((TOK, CHAN), F32),
            shape((TOK, HEADS), F32),
            shape((HEADS, TOK), F32),
        ),
        1_000_000_000,
    )(values, in_map, log_decay)


def silu_parts(x):
    squash = jax.nn.sigmoid(x)
    return x * squash, squash * (1.0 + x * (1.0 - squash))


def expert_body(
    tp, own, peer, gate_o, gate_p, up_o, up_p, down_o, down_p,
    rows_s, cot_s, active, pre_grad, up_grad, part_o, part_p, acc_o, acc_p,
):
    step = pl.program_id(0)

    @pl.when(step == 0)
    def _():
        for i, got in enumerate((own, peer)):
            rows_s[i, :MAIN] = got[:, 0:HALF]
            cot_s[i, :MAIN] = got[:, HALF : 2 * HALF]
            last_rows, last_cot = unfold_last(got[:, 2 * HALF :])
            rows_s[i, MAIN:] = last_rows
            cot_s[i, MAIN:] = last_cot

    gate_pre = mm(rows_s[0], gate_o[0], NN) + mm(rows_s[1], gate_p[0], NN)
    up_val = mm(rows_s[0], up_o[0], NN) + mm(rows_s[1], up_p[0], NN)
    act_grad = mm(cot_s[0], down_o[0], NT) + mm(cot_s[1], down_p[0], NT)
    act, slope = silu_parts(gate_pre)
    active[...] = (act * up_val).astype(BF)
    up_g = (act_grad * act).astype(BF)
    pre_g = (act_grad * up_val * slope).astype(BF)
    up_grad[...] = up_g
    pre_grad[...] = pre_g
    new_o = mm(pre_g, gate_o[0], NT) + mm(up_g, up_o[0], NT)
    new_p = mm(pre_g, gate_p[0], NT) + mm(up_g, up_p[0], NT)

    @pl.when(step == 0)
    def _():
        acc_o[...] = new_o
        acc_p[...] = new_p

    @pl.when(step == 1)
    def _():
        acc_o[...] += new_o
        acc_p[...] += new_p

    @pl.when(step == 2)
    def _():
        part_o[...] = (acc_o[...] + new_o).astype(BF)
        part_p[...] = (acc_p[...] + new_p).astype(BF)


def expert(tp, own, peer, gate_w, up_w, down_w):
    wide = 2 * HALF + 256
    spec = pltpu.PrefetchScalarGridSpec(
        num_scalar_prefetch=1,
        grid=(FF // FF_STEP,),
        in_specs=[
            whole((MAIN, wide)),
            whole((MAIN, wide)),
            pl.BlockSpec((1, HALF, FF_STEP), lambda i, t: (0, t[0], i)),
            pl.BlockSpec((1, HALF, FF_STEP), lambda i, t: (0, 1 - t[0], i)),
            pl.BlockSpec((1, HALF, FF_STEP), lambda i, t: (0, t[0], i)),
            pl.BlockSpec((1, HALF, FF_STEP), lambda i, t: (0, 1 - t[0], i)),
            pl.BlockSpec((1, FF_STEP, HALF), lambda i, t: (0, i, t[0])),
            pl.BlockSpec((1, FF_STEP, HALF), lambda i, t: (0, i, 1 - t[0])),
        ],
        out_specs=[
            whole((2, SLOTS, HALF)),
            whole((2, SLOTS, HALF)),
            pl.BlockSpec((SLOTS, FF_STEP), lambda i, t: (0, i)),
            pl.BlockSpec((SLOTS, FF_STEP), lambda i, t: (0, i)),
            pl.BlockSpec((SLOTS, FF_STEP), lambda i, t: (0, i)),
            whole((SLOTS, HALF)),
            whole((SLOTS, HALF)),
        ],
        scratch_shapes=[pltpu.VMEM((SLOTS, HALF), F32), pltpu.VMEM((SLOTS, HALF), F32)],
    )
    return call(
        expert_body,
        "expert",
        (
            shape((2, SLOTS, HALF)),
            shape((2, SLOTS, HALF)),
            shape((SLOTS, FF)),
            shape((SLOTS, FF)),
            shape((SLOTS, FF)),
            shape((SLOTS, HALF)),
            shape((SLOTS, HALF)),
        ),
        9_000_000_000,
        grid_spec=spec,
    )(tp, own, peer, gate_w, gate_w, up_w, up_w, down_w, down_w)


def weight_body(tp, rows, cot, active, pre_grad, up_grad, gate_g, up_g, down_g):
    gate_g[0] = mm(rows[0], pre_grad[...], TN).astype(BF)
    up_g[0] = mm(rows[0], up_grad[...], TN).astype(BF)
    down_g[0] = mm(active[...], cot[0], TN).astype(BF)


def weight_grads(tp, rows_s, cot_s, active, pre_grad, up_grad):
    quarter = HALF // 2

    def block(i, t):
        return (t[0] * (1 - i // 2) + (1 - t[0]) * (i // 2)) * 2 + i % 2

    spec = pltpu.PrefetchScalarGridSpec(
        num_scalar_prefetch=1,
        grid=(4,),
        in_specs=[
            pl.BlockSpec((1, SLOTS, quarter), lambda i, t: (i // 2, 0, i % 2)),
            pl.BlockSpec((1, SLOTS, quarter), lambda i, t: (i // 2, 0, i % 2)),
            whole((SLOTS, FF)),
            whole((SLOTS, FF)),
            whole((SLOTS, FF)),
        ],
        out_specs=[
            pl.BlockSpec((1, quarter, FF), lambda i, t: (0, block(i, t), 0)),
            pl.BlockSpec((1, quarter, FF), lambda i, t: (0, block(i, t), 0)),
            pl.BlockSpec((1, FF, quarter), lambda i, t: (0, 0, block(i, t))),
        ],
    )
    return call(
        weight_body,
        "weight_grads",
        (shape((1, WIDTH, FF)), shape((1, WIDTH, FF)), shape((1, FF, WIDTH))),
        5_400_000_000,
        grid_spec=spec,
    )(tp, rows_s, cot_s, active, pre_grad, up_grad)


def reply_body(own, peer, states, out):
    total = (own[...].astype(F32) + peer[...].astype(F32)).astype(BF)
    out[:, 0:HALF] = total[:MAIN]
    out[:, HALF : HALF + 128] = fold_last(total[MAIN:])
    out[:, HALF + 128 :] = states[...]


def reply(own, peer, states):
    return call(reply_body, "reply", shape((MAIN, HALF + 128 + 384)), 100_000_000)(
        own, peer, states
    )


def scan_states(left_in, right_in, decays, out, work):
    def factor(b):
        at = 8 * b
        return decays[at : at + 1] + decays[at + 1 : at + 2] + decays[at + 2 : at + 3]

    factors = [factor(b) for b in range(BLOCKS)]
    left = jnp.zeros((8, 128), F32)
    right = jnp.zeros((8, 128), F32)
    for b in range(BLOCKS):
        at = 8 * b
        work[at : at + 8, 0:128] = left
        left = factors[b] * left + left_in[at : at + 8]
        back = BLOCKS - 1 - b
        at = 8 * back
        work[at : at + 8, 128:256] = right
        right = factors[back] * right + right_in[at : at + 8]
    out[...] = work[...].astype(BF)


def join_body(tp, got, ids, cot, out, states, decays, work, wide):
    first, second = slot_choices(ids[...])
    both = ones_where(first | second)
    (last,) = unfold_last(got[:, HALF : HALF + 128])
    total = mm(both[:, :MAIN], got[:, :HALF], NN) + mm(both[:, MAIN:], last, NN)
    out[...] = (cot[...].astype(F32) + total).astype(BF)
    wide[...] = got[:, HALF + 128 :].astype(F32)
    decays[...] = wide[:, 256:]
    scan_states(wide[:, 0:128], wide[:, 128:256], wide[:, 256:], states, work)


def join(tp, got, ids, cot):
    spec = pltpu.PrefetchScalarGridSpec(
        num_scalar_prefetch=1,
        grid=(1,),
        in_specs=[
            whole((MAIN, HALF + 512)),
            whole((TOK, 2)),
            pl.BlockSpec((TOK, HALF), lambda i, t: (0, t[0])),
        ],
        out_specs=[whole((TOK, HALF)), whole((MAIN, 256)), whole((MAIN, 128))],
        scratch_shapes=[pltpu.VMEM((MAIN, 256), F32), pltpu.VMEM((MAIN, 384), F32)],
    )
    return call(
        join_body,
        "join",
        (shape((TOK, HALF)), shape((MAIN, 256)), shape((MAIN, 128), F32)),
        300_000_000,
        grid_spec=spec,
    )(tp, got, ids, cot)


def mix_body(
    stream, proj_w, gate_in, scan_out, start_w, end_w, out_map, x_states,
    gate_grad, scan_grad, gated, payload,
):
    mixed = mm(stream[0], proj_w[:, :HALF], NT) + mm(stream[1], proj_w[:, HALF:], NT)
    scan = scan_out[...].astype(F32)
    act, slope = silu_parts(gate_in[...].astype(F32))
    gated[...] = (scan * act).astype(BF)
    gate_grad[...] = (mixed * scan * slope).astype(BF)
    grad = (mixed * act).astype(BF)
    scan_grad[...] = grad
    wide = grad.astype(F32)
    block_states(
        payload, (end_w[...] * wide).astype(BF), (start_w[...] * wide).astype(BF), out_map
    )
    payload[:, 256:] = x_states[...]


def mix(*args):
    return call(
        mix_body,
        "mix",
        (shape((TOK, CHAN)), shape((TOK, CHAN)), shape((TOK, CHAN)), shape((MAIN, 512))),
        500_000_000,
    )(*args)


def proj_body(stream, gated, out):
    out[:HALF] = mm(stream[0], gated[...], TN).astype(BF)
    out[HALF:] = mm(stream[1], gated[...], TN).astype(BF)


def proj_part(stream, gated):
    return call(proj_body, "proj_part", shape((WIDTH, CHAN)), 400_000_000)(stream, gated)


def scan_body(got, decays, out, work, wide):
    wide[...] = got[:, 0:256].astype(F32)
    scan_states(wide[:, 0:128], wide[:, 128:256], decays[...], out, work)


def scan_grads(got, decays):
    return call(
        scan_body,
        "scan_grads",
        shape((MAIN, 256)),
        100_000_000,
        scratch_shapes=[pltpu.VMEM((MAIN, 256), F32), pltpu.VMEM((MAIN, 256), F32)],
    )(got, decays)


def near_body(
    scan_grad, values, in_map, out_map, cum, cum_t, start_w, end_w, states,
    out_grad, value_part, in_part,
):
    wide = scan_grad[...].astype(F32)
    from_start = (start_w[...] * wide).astype(BF)
    to_end = (end_w[...] * wide).astype(BF)
    for g in range(2):
        keys = slice(128 * g, 128 * g + 128)
        chan = slice(256 * g, 256 * g + 256)
        in_keys = in_map[:, keys]
        out_keys = out_map[:, keys]
        meet = mm(out_keys, in_keys, NT)
        pair_sum = jnp.zeros((TOK, TOK), F32)
        for e in range(4):
            h = 4 * g + e
            at = slice(64 * h, 64 * h + 64)
            kernel = jnp.exp(-jnp.abs(cum[:, h : h + 1] - cum_t[h : h + 1, :]))
            grad = scan_grad[:, at]
            value_part[:, at] = mm((kernel * meet).astype(BF), grad, TN)
            pair_sum = pair_sum + kernel * mm(grad, values[:, at], NT)
        pair_sum = pair_sum.astype(BF)
        out_total = mm(pair_sum, in_keys, NN)
        out_total = out_total + mm(from_start[:, chan], states[chan, 0:128], NN)
        out_total = out_total + mm(to_end[:, chan], states[chan, 128:256], NN)
        out_grad[:, keys] = out_total.astype(BF)
        in_part[:, keys] = mm(pair_sum, out_keys, TN)


def near(*args):
    return call(
        near_body,
        "near",
        (shape((TOK, KEYS)), shape((TOK, CHAN), F32), shape((TOK, KEYS), F32)),
        600_000_000,
    )(*args)


def far_body(states, values, in_map, start_w, end_w, value_part, in_part, value_grad, in_grad):
    val = values[...].astype(F32)
    from_start = (start_w[...] * val).astype(BF)
    to_end = (end_w[...] * val).astype(BF)
    for g in range(2):
        keys = slice(128 * g, 128 * g + 128)
        chan = slice(256 * g, 256 * g + 256)
        in_keys = in_map[:, keys]
        left = states[chan, 0:128]
        right = states[chan, 128:256]
        total = value_part[:, chan] + start_w[:, chan] * mm(in_keys, left, NT)
        total = total + end_w[:, chan] * mm(in_keys, right, NT)
        value_grad[:, chan] = total.astype(BF)
        total = in_part[:, keys] + mm(from_start[:, chan], left, NN)
        total = total + mm(to_end[:, chan], right, NN)
        in_grad[:, keys] = total.astype(BF)


def far(*args):
    return call(far_body, "far", (shape((TOK, CHAN)), shape((TOK, KEYS))), 200_000_000)(*args)


def swap(rows):
    lanes = rows.shape[1]
    out = lax.all_to_all(rows.reshape(BLOCKS, -1, lanes), SP, 0, 0, tiled=True)
    return out.reshape(-1, lanes)


def other_core(array):
    return lax.ppermute(array, "tp", [(0, 1), (1, 0)])


def on_device(
    stream_rows,
    out_cotangent,
    expert_ids,
    route_weights,
    gate_weight,
    up_weight,
    down_weight,
    proj_weight,
    gate_input,
    scan_out,
    values,
    in_map,
    out_map,
    log_decay,
):
    tp = lax.axis_index("tp").astype(jnp.int32).reshape(1)
    sent = pack(tp, expert_ids, route_weights, stream_rows, out_cotangent)
    own = swap(sent)
    x_payload, start_w, end_w, cum, cum_t = decay(values, in_map, log_decay)
    peer = other_core(own)
    rows_s, cot_s, active, pre_grad, up_grad, part_own, part_peer = expert(
        tp, own, peer, gate_weight, up_weight, down_weight
    )
    back = swap(reply(part_own, other_core(part_peer), x_payload))
    gate_w_grad, up_w_grad, down_grad = weight_grads(
        tp, rows_s, cot_s, active, pre_grad, up_grad
    )
    stream_grad, x_states, decays = join(tp, back, expert_ids, out_cotangent)
    stream = lax.all_gather(stream_grad, "tp")
    gate_grad, scan_grad, gated, payload = mix(
        stream, proj_weight, gate_input, scan_out, start_w, end_w, out_map, x_states
    )
    got = swap(payload)
    g_states = swap(scan_grads(got, decays))
    partial = swap(proj_part(stream, gated))
    proj_grad = jnp.sum(partial.reshape(BLOCKS, 32, CHAN).astype(F32), axis=0)
    out_grad, value_part, in_part = near(
        scan_grad, values, in_map, out_map, cum, cum_t, start_w, end_w, got[:, 256:]
    )
    value_grad, in_grad = far(g_states, values, in_map, start_w, end_w, value_part, in_part)
    return (
        stream_grad,
        proj_grad,
        value_grad,
        in_grad,
        out_grad,
        gate_grad,
        gate_w_grad,
        up_w_grad,
        down_grad,
    )


def solution(mesh):
    finer = Mesh(mesh.devices.reshape(4, 4, 4, mesh.shape["tp"]), ("sp_0", "sp_1", "sp_2", "tp"))
    return jax.shard_map(
        on_device,
        mesh=finer,
        in_specs=(
            P(SP, None),
            P(SP, None),
            P(SP, None),
            P(SP, None),
            P(SP, None, "tp"),
            P(SP, None, "tp"),
            P(SP, "tp", None),
            P("tp", None),
            P(SP, "tp"),
            P(SP, "tp"),
            P(SP, "tp"),
            P(SP, "tp"),
            P(SP, "tp"),
            P(SP, "tp"),
        ),
        out_specs=(
            P(SP, "tp"),
            P(SP, "tp"),
            P(SP, "tp"),
            P(SP, "tp"),
            P(SP, "tp"),
            P(SP, "tp"),
            P(SP, None, "tp"),
            P(SP, None, "tp"),
            P(SP, "tp", None),
        ),
        check_vma=False,
    )
```

```python
import jax
import jax.numpy as jnp
from jax import lax
from jax.experimental import pallas as pl
from jax.experimental.pallas import tpu as pltpu
from jax.sharding import Mesh
from jax.sharding import PartitionSpec as P


SP = ("sp_0", "sp_1", "sp_2")
TOK = 192
WIDTH = 2048
HALF = 1024
EXPERTS = 64
MAIN = 512
SLOTS = 576
FF = 768
FF_STEP = 256
CHAN = 512
KEYS = 256
HEADS = 8
BLOCKS = 64

BF = jnp.bfloat16
F32 = jnp.float32
EXACT = lax.Precision.HIGHEST


def mm(a, b, dims, precision=None):
    return lax.dot_general(a, b, (dims, ((), ())), preferred_element_type=F32, precision=precision)


NN = ((1,), (0,))
NT = ((1,), (1,))
TN = ((0,), (0,))


def iota(shape, dim):
    return lax.broadcasted_iota(jnp.int32, shape, dim)


def ones_where(mask):
    return jnp.where(mask, 1.0, 0.0).astype(BF)


def call(body, out_shape, flops, hbm_in=(), **kw):
    vmem = kw.pop("vmem", 12 << 20)
    kernel = pl.pallas_call(
        body,
        out_shape=out_shape,
        compiler_params=pltpu.CompilerParams(vmem_limit_bytes=vmem),
        cost_estimate=pl.CostEstimate(flops=flops, bytes_accessed=1 << 20, transcendentals=0),
        **kw,
    )

    def run(*args):
        return kernel(
            *[
                pltpu.with_memory_space_constraint(a, pltpu.HBM) if i in hbm_in else a
                for i, a in enumerate(args)
            ]
        )

    return run


def shape(dims, dtype=BF):
    return jax.ShapeDtypeStruct(dims, dtype)


def slot_choices(ids):
    expert = iota((EXPERTS, TOK), 0)
    named = [ids[k : k + 1] == expert for k in range(2)]
    either = ones_where(named[0] | named[1])
    earlier = ones_where(iota((TOK, TOK), 0) < iota((TOK, TOK), 1))
    count = mm(either, earlier, NN)
    picks = []
    for k in range(2):
        rank = jnp.sum(jnp.where(named[k], count, 0.0), axis=0, keepdims=True).astype(jnp.int32)
        own = ids[k : k + 1]
        row = jnp.where(rank < 8, own * 8 + rank, MAIN + own)
        picks.append(row == iota((SLOTS, TOK), 0))
    return picks


def fold_last(rows):
    q = iota((MAIN, MAIN), 0)
    order = ones_where(iota((MAIN, MAIN), 1) == (q & 7) * EXPERTS + (q >> 3))
    stacked = jnp.concatenate([rows[:, 128 * j : 128 * j + 128] for j in range(8)], axis=0)
    return mm(order, stacked, NN).astype(BF)


def unfold_last(folded):
    c = iota((MAIN, MAIN), 0)
    order = ones_where(iota((MAIN, MAIN), 1) == (c & 63) * 8 + (c >> 6))
    stacked = mm(order, folded, NN).astype(BF)
    return [
        jnp.concatenate(
            [stacked[64 * j : 64 * j + 64, 128 * i : 128 * i + 128] for j in range(8)], axis=1
        )
        for i in range(folded.shape[1] // 128)
    ]


def pack_body(tp, ids, weights, rows_hbm, cot_hbm, out, rows, cot, sems):
    at = pl.ds(pl.multiple_of(tp[0] * HALF, HALF), HALF)
    get_rows = pltpu.make_async_copy(rows_hbm.at[:, at], rows, sems.at[0])
    get_cot = pltpu.make_async_copy(cot_hbm.at[:, at], cot, sems.at[1])
    get_rows.start()
    get_cot.start()
    first, second = slot_choices(ids[...])
    both = ones_where(first | second)
    same = iota((TOK, TOK), 0) == iota((TOK, TOK), 1)

    def column(k):
        return jnp.sum(jnp.where(same, weights[k : k + 1], 0.0), axis=1, keepdims=True)

    get_rows.wait()
    row_slots = mm(both, rows[...], NN).astype(BF)
    out[:, 0:HALF] = row_slots[:MAIN]
    out[:, 2 * HALF : 2 * HALF + 128] = fold_last(row_slots[MAIN:])
    get_cot.wait()
    full = cot[...].astype(F32)
    cot_slots = mm(ones_where(first), (column(0) * full).astype(BF), NN)
    cot_slots = cot_slots + mm(ones_where(second), (column(1) * full).astype(BF), NN)
    cot_slots = cot_slots.astype(BF)
    out[:, HALF : 2 * HALF] = cot_slots[:MAIN]
    out[:, 2 * HALF + 128 :] = fold_last(cot_slots[MAIN:])


def whole(dims):
    return pl.BlockSpec(dims, lambda *_: (0,) * len(dims))


def pack(tp, ids, weights, rows, cot):
    spec = pltpu.PrefetchScalarGridSpec(
        num_scalar_prefetch=1,
        grid=(1,),
        in_specs=[
            whole((2, TOK)),
            whole((2, TOK)),
            pl.BlockSpec(memory_space=pltpu.HBM),
            pl.BlockSpec(memory_space=pltpu.HBM),
        ],
        out_specs=whole((MAIN, 2 * HALF + 256)),
        scratch_shapes=[
            pltpu.VMEM((TOK, HALF), BF),
            pltpu.VMEM((TOK, HALF), BF),
            pltpu.SemaphoreType.DMA((2,)),
        ],
    )
    return call(
        pack_body, shape((MAIN, 2 * HALF + 256)), 1_000_000_000, hbm_in=(1, 2, 3, 4), grid_spec=spec
    )(tp, ids, weights, rows, cot)


def decay_body(values, in_map, log_decay, payload, start_w, end_w, cum_out, cum_t_out):
    upto = jnp.where(iota((TOK, TOK), 0) <= iota((TOK, TOK), 1), 1.0, 0.0)
    cum = mm(upto, log_decay[...], ((0,), (1,)), EXACT)
    cum_t = mm(log_decay[...], upto, NN, EXACT)
    cum_out[...] = cum
    cum_t_out[...] = cum_t
    spread = jnp.where(iota((HEADS, CHAN), 1) // 64 == iota((HEADS, CHAN), 0), 1.0, 0.0)
    from_start = mm(jnp.exp(cum), spread, NN, EXACT)
    to_end = mm(jnp.exp(cum[TOK - 1 :, :] - cum), spread, NN, EXACT)
    start_w[...] = from_start
    end_w[...] = to_end
    val = values[...].astype(F32)
    block_states(payload, (to_end * val).astype(BF), (from_start * val).astype(BF), in_map)
    total = jnp.exp(cum_t[:, TOK - 1 :])
    total = jnp.concatenate(
        [jnp.broadcast_to(total[h : h + 1], (64, 128)) for h in range(HEADS)], axis=0
    )
    high = total.astype(BF)
    rest = total - high.astype(F32)
    mid = rest.astype(BF)
    low = (rest - mid.astype(F32)).astype(BF)
    part = iota((MAIN, 128), 0) & 7
    parts = jnp.where(part == 0, high.astype(F32), 0.0)
    parts = jnp.where(part == 1, mid.astype(F32), parts)
    parts = jnp.where(part == 2, low.astype(F32), parts)
    payload[:, 256:] = parts.astype(BF)


def block_states(payload, to_end, from_start, keys):
    for g in range(2):
        chan = slice(256 * g, 256 * g + 256)
        key = keys[:, 128 * g : 128 * g + 128]
        payload[chan, 0:128] = mm(to_end[:, chan], key, TN).astype(BF)
        payload[chan, 128:256] = mm(from_start[:, chan], key, TN).astype(BF)


def decay(values, in_map, log_decay):
    return call(
        decay_body,
        (
            shape((MAIN, 384)),
            shape((TOK, CHAN), F32),
            shape((TOK, CHAN), F32),
            shape((TOK, HEADS), F32),
            shape((HEADS, TOK), F32),
        ),
        1_000_000_000,
    )(values, in_map, log_decay)


def silu_parts(x):
    squash = 0.5 * jnp.tanh(0.5 * x) + 0.5
    return x * squash, squash * (1.0 + x * (1.0 - squash))


def split_slots(got, rows, cot):
    rows[:MAIN] = got[:, 0:HALF]
    cot[:MAIN] = got[:, HALF : 2 * HALF]
    last_rows, last_cot = unfold_last(got[:, 2 * HALF :])
    rows[MAIN:] = last_rows
    cot[MAIN:] = last_cot


def own_body(tp, own, gate_w, up_w, down_w, rows, cot, gate_o, up_o, act_o):
    @pl.when(pl.program_id(0) == 0)
    def _():
        split_slots(own, rows, cot)

    gate_o[...] = mm(rows[...], gate_w[0], NN)
    up_o[...] = mm(rows[...], up_w[0], NN)
    act_o[...] = mm(cot[...], down_w[0], NT)


def step_block(dims):
    return pl.BlockSpec(dims, lambda i, t: (0, i))


def expert_own(tp, own, gate_w, up_w, down_w):
    spec = pltpu.PrefetchScalarGridSpec(
        num_scalar_prefetch=1,
        grid=(FF // FF_STEP,),
        in_specs=[
            whole((MAIN, 2 * HALF + 256)),
            pl.BlockSpec((1, HALF, FF_STEP), lambda i, t: (0, t[0], i)),
            pl.BlockSpec((1, HALF, FF_STEP), lambda i, t: (0, t[0], i)),
            pl.BlockSpec((1, FF_STEP, HALF), lambda i, t: (0, i, t[0])),
        ],
        out_specs=[whole((SLOTS, HALF))] * 2 + [step_block((SLOTS, FF_STEP))] * 3,
    )
    return call(
        own_body,
        [shape((SLOTS, HALF))] * 2 + [shape((SLOTS, FF), F32)] * 3,
        2_700_000_000,
        hbm_in=(2, 3, 4),
        grid_spec=spec,
        vmem=24 << 20,
    )(tp, own, gate_w, up_w, down_w)


def peer_body(
    tp, peer, gate_w, up_w, down_w, gate_o, up_o, act_o,
    rows, cot, active, pre_grad, up_grad, part, acc,
):
    step = pl.program_id(0)

    @pl.when(step == 0)
    def _():
        split_slots(peer, rows, cot)

    gate_pre = gate_o[...] + mm(rows[...], gate_w[0], NN)
    up_val = up_o[...] + mm(rows[...], up_w[0], NN)
    act_grad = act_o[...] + mm(cot[...], down_w[0], NT)
    act, slope = silu_parts(gate_pre)
    active[...] = (act * up_val).astype(BF)
    up_g = (act_grad * act).astype(BF)
    pre_g = (act_grad * up_val * slope).astype(BF)
    up_grad[...] = up_g
    pre_grad[...] = pre_g
    new = mm(pre_g, gate_w[0], NT) + mm(up_g, up_w[0], NT)

    @pl.when(step == 0)
    def _():
        acc[...] = new

    @pl.when(step == 1)
    def _():
        acc[...] += new

    @pl.when(step == 2)
    def _():
        part[...] = (acc[...] + new).astype(BF)


def expert_peer(tp, peer, gate_w, up_w, down_w, gate_o, up_o, act_o):
    spec = pltpu.PrefetchScalarGridSpec(
        num_scalar_prefetch=1,
        grid=(FF // FF_STEP,),
        in_specs=[
            whole((MAIN, 2 * HALF + 256)),
            pl.BlockSpec((1, HALF, FF_STEP), lambda i, t: (0, 1 - t[0], i)),
            pl.BlockSpec((1, HALF, FF_STEP), lambda i, t: (0, 1 - t[0], i)),
            pl.BlockSpec((1, FF_STEP, HALF), lambda i, t: (0, i, 1 - t[0])),
        ]
        + [step_block((SLOTS, FF_STEP))] * 3,
        out_specs=[whole((SLOTS, HALF))] * 2
        + [step_block((SLOTS, FF_STEP))] * 3
        + [whole((SLOTS, HALF))],
        scratch_shapes=[pltpu.VMEM((SLOTS, HALF), F32)],
    )
    return call(
        peer_body,
        [shape((SLOTS, HALF))] * 2 + [shape((SLOTS, FF))] * 3 + [shape((SLOTS, HALF))],
        4_500_000_000,
        hbm_in=(2, 3, 4),
        grid_spec=spec,
        vmem=28 << 20,
    )(tp, peer, gate_w, up_w, down_w, gate_o, up_o, act_o)


def rows_body(tp, pre_grad, up_grad, gate_w, up_w, part):
    total = mm(pre_grad[...], gate_w[0], NT) + mm(up_grad[...], up_w[0], NT)
    part[...] = total.astype(BF)


def own_rows(tp, pre_grad, up_grad, gate_w, up_w):
    spec = pltpu.PrefetchScalarGridSpec(
        num_scalar_prefetch=1,
        grid=(4,),
        in_specs=[
            whole((SLOTS, FF)),
            whole((SLOTS, FF)),
            pl.BlockSpec((1, HALF // 4, FF), lambda i, t: (0, 4 * t[0] + i, 0)),
            pl.BlockSpec((1, HALF // 4, FF), lambda i, t: (0, 4 * t[0] + i, 0)),
        ],
        out_specs=step_block((SLOTS, HALF // 4)),
    )
    return call(
        rows_body, shape((SLOTS, HALF)), 1_800_000_000, grid_spec=spec, vmem=12 << 20
    )(tp, pre_grad, up_grad, gate_w, up_w)


def weight_body(tp, rows_o, cot_o, rows_p, cot_p, active, pre_grad, up_grad, gate_g, up_g, down_g):
    for half, rows, cot in ((0, rows_o, cot_o), (1, rows_p, cot_p)):

        @pl.when(pl.program_id(0) // 2 == half)
        def _():
            gate_g[0] = mm(rows[...], pre_grad[...], TN).astype(BF)
            up_g[0] = mm(rows[...], up_grad[...], TN).astype(BF)
            down_g[0] = mm(active[...], cot[...], TN).astype(BF)


def weight_grads(tp, rows_o, cot_o, rows_p, cot_p, active, pre_grad, up_grad):
    quarter = HALF // 2

    def block(i, t):
        return (t[0] * (1 - i // 2) + (1 - t[0]) * (i // 2)) * 2 + i % 2

    spec = pltpu.PrefetchScalarGridSpec(
        num_scalar_prefetch=1,
        grid=(4,),
        in_specs=[pl.BlockSpec((SLOTS, quarter), lambda i, t: (0, i % 2))] * 4
        + [whole((SLOTS, FF))] * 3,
        out_specs=[
            pl.BlockSpec((1, quarter, FF), lambda i, t: (0, block(i, t), 0)),
            pl.BlockSpec((1, quarter, FF), lambda i, t: (0, block(i, t), 0)),
            pl.BlockSpec((1, FF, quarter), lambda i, t: (0, 0, block(i, t))),
        ],
    )
    return call(
        weight_body,
        (shape((1, WIDTH, FF)), shape((1, WIDTH, FF)), shape((1, FF, WIDTH))),
        5_400_000_000,
        grid_spec=spec,
        vmem=24 << 20,
    )(tp, rows_o, cot_o, rows_p, cot_p, active, pre_grad, up_grad)


def reply_body(own, peer, states, out):
    total = (own[...].astype(F32) + peer[...].astype(F32)).astype(BF)
    out[:, 0:HALF] = total[:MAIN]
    out[:, HALF : HALF + 128] = fold_last(total[MAIN:])
    out[:, HALF + 128 :] = states[...]


def reply(own, peer, states):
    return call(reply_body, shape((MAIN, HALF + 128 + 384)), 100_000_000)(own, peer, states)


def scan_states(left_in, right_in, decays, out, work):
    def factor(b):
        at = 8 * b
        return decays[at : at + 1] + decays[at + 1 : at + 2] + decays[at + 2 : at + 3]

    factors = [factor(b) for b in range(BLOCKS)]
    left = jnp.zeros((8, 128), F32)
    right = jnp.zeros((8, 128), F32)
    for b in range(BLOCKS):
        at = 8 * b
        work[at : at + 8, 0:128] = left
        left = factors[b] * left + left_in[at : at + 8]
        back = BLOCKS - 1 - b
        at = 8 * back
        work[at : at + 8, 128:256] = right
        right = factors[back] * right + right_in[at : at + 8]
    out[:, 0:256] = work[...].astype(BF)


def join_body(tp, got, ids, cot, out, states, decays, work, wide):
    first, second = slot_choices(ids[...])
    both = ones_where(first | second)
    (last,) = unfold_last(got[:, HALF : HALF + 128])
    total = mm(both[:MAIN], got[:, :HALF], TN) + mm(both[MAIN:], last, TN)
    out[...] = (cot[...].astype(F32) + total).astype(BF)
    wide[...] = got[:, HALF + 128 :].astype(F32)
    decays[...] = wide[:, 256:]
    scan_states(wide[:, 0:128], wide[:, 128:256], wide[:, 256:], states, work)


def join(tp, got, ids, cot):
    spec = pltpu.PrefetchScalarGridSpec(
        num_scalar_prefetch=1,
        grid=(1,),
        in_specs=[
            whole((MAIN, HALF + 512)),
            whole((2, TOK)),
            pl.BlockSpec((TOK, HALF), lambda i, t: (0, t[0])),
        ],
        out_specs=[whole((TOK, HALF)), whole((MAIN, 256)), whole((MAIN, 128))],
        scratch_shapes=[pltpu.VMEM((MAIN, 256), F32), pltpu.VMEM((MAIN, 384), F32)],
    )
    return call(
        join_body,
        (shape((TOK, HALF)), shape((MAIN, 256)), shape((MAIN, 128), F32)),
        300_000_000,
        grid_spec=spec,
    )(tp, got, ids, cot)


def mix_body(
    stream, proj_w, gate_in, scan_out, start_w, end_w, out_map, x_states,
    gate_grad, scan_grad, gated, payload,
):
    mixed = mm(stream[0], proj_w[:, :HALF], NT) + mm(stream[1], proj_w[:, HALF:], NT)
    scan = scan_out[...].astype(F32)
    act, slope = silu_parts(gate_in[...].astype(F32))
    gated[...] = (scan * act).astype(BF)
    gate_grad[...] = (mixed * scan * slope).astype(BF)
    grad = (mixed * act).astype(BF)
    scan_grad[...] = grad
    wide = grad.astype(F32)
    block_states(
        payload, (end_w[...] * wide).astype(BF), (start_w[...] * wide).astype(BF), out_map
    )
    payload[:, 256:] = x_states[...]


def mix(*args):
    return call(
        mix_body,
        (shape((TOK, CHAN)), shape((TOK, CHAN)), shape((TOK, CHAN)), shape((MAIN, 512))),
        500_000_000,
    )(*args)


PARTS = ((0, 384), (768, 384), (1536, 256))


def proj_body(odd, stream, gated, keep, *sends):
    for i in range(2):
        part = mm(stream[i], gated[...], TN).reshape(32, 4, 8, CHAN)
        flat = [part[:, q].reshape(256, CHAN) for q in range(4)]
        rows = slice(256 * i, 256 * i + 256)

        def tile(t):
            return flat[t // 4][:, 128 * (t % 4) : 128 * (t % 4) + 128]

        at = 0
        for j, (first, width) in enumerate(PARTS):
            for k in range(width // 128):
                low = tile(first // 128 + k)
                high = tile((first + width) // 128 + k)
                upper = odd[j] == 1
                keep[rows, at : at + 128] = jnp.where(upper, high, low).astype(BF)
                sends[j][rows, 128 * k : 128 * k + 128] = jnp.where(upper, low, high).astype(BF)
                at += 128


def proj_part(odd, stream, gated):
    out = [shape((MAIN, 1024))] + [shape((MAIN, width)) for _, width in PARTS]
    spec = pltpu.PrefetchScalarGridSpec(
        num_scalar_prefetch=1,
        grid=(1,),
        in_specs=[whole((2, TOK, HALF)), whole((TOK, CHAN))],
        out_specs=[whole(o.shape) for o in out],
    )
    return call(proj_body, out, 400_000_000, grid_spec=spec)(odd, stream, gated)


def scan_body(got, decays, keep, first, second, third, out, work, wide):
    at = 0
    for other in (first, second, third):
        width = other.shape[1]
        total = keep[:, at : at + width].astype(F32) + other[...].astype(F32)
        out[:, 256 + at : 256 + at + width] = total.astype(BF)
        at += width
    wide[...] = got[:, 0:256].astype(F32)
    scan_states(wide[:, 0:128], wide[:, 128:256], decays[...], out, work)


def scan_grads(got, decays, keep, others):
    spec = pl.GridSpec(
        grid=(1,),
        in_specs=[whole((MAIN, 512)), whole((MAIN, 128)), whole((MAIN, 1024))]
        + [whole(o.shape) for o in others],
        out_specs=whole((MAIN, 256 + 1024)),
        scratch_shapes=[pltpu.VMEM((MAIN, 256), F32), pltpu.VMEM((MAIN, 256), F32)],
    )
    return call(
        scan_body, shape((MAIN, 256 + 1024)), 100_000_000, grid_spec=spec
    )(got, decays, keep, *others)


def near_body(
    scan_grad, values, in_map, out_map, cum, cum_t, start_w, end_w, states,
    out_grad, value_part, in_part,
):
    wide = scan_grad[...].astype(F32)
    from_start = (start_w[...] * wide).astype(BF)
    to_end = (end_w[...] * wide).astype(BF)
    for g in range(2):
        keys = slice(128 * g, 128 * g + 128)
        chan = slice(256 * g, 256 * g + 256)
        in_keys = in_map[:, keys]
        out_keys = out_map[:, keys]
        meet = mm(out_keys, in_keys, NT)
        pair_sum = jnp.zeros((TOK, TOK), F32)
        for e in range(4):
            h = 4 * g + e
            at = slice(64 * h, 64 * h + 64)
            kernel = jnp.exp(-jnp.abs(cum[:, h : h + 1] - cum_t[h : h + 1, :]))
            grad = scan_grad[:, at]
            value_part[:, at] = mm((kernel * meet).astype(BF), grad, TN)
            pair_sum = pair_sum + kernel * mm(grad, values[:, at], NT)
        pair_sum = pair_sum.astype(BF)
        out_total = mm(pair_sum, in_keys, NN)
        out_total = out_total + mm(from_start[:, chan], states[chan, 0:128], NN)
        out_total = out_total + mm(to_end[:, chan], states[chan, 128:256], NN)
        out_grad[:, keys] = out_total.astype(BF)
        in_part[:, keys] = mm(pair_sum, out_keys, TN)


def near(*args):
    return call(
        near_body,
        (shape((TOK, KEYS)), shape((TOK, CHAN), F32), shape((TOK, KEYS), F32)),
        600_000_000,
    )(*args)


def far_body(
    states, values_h, in_map_h, start_h, end_h, value_part_h, in_part_h,
    value_grad, in_grad, proj_grad,
    values, in_map, start_w, end_w, value_part, in_part, sems,
):
    pairs = (
        (values_h, values),
        (in_map_h, in_map),
        (start_h, start_w),
        (end_h, end_w),
        (value_part_h, value_part),
        (in_part_h, in_part),
    )
    copies = [pltpu.make_async_copy(a, b, sems.at[i]) for i, (a, b) in enumerate(pairs)]
    for c in copies:
        c.start()
    at = 256
    for j, (first, width) in enumerate(PARTS):
        sums = [jnp.zeros((8, width), F32), jnp.zeros((8, width), F32)]
        for b in range(BLOCKS):
            half = (b >> (4 - 2 * j)) & 1
            sums[half] = sums[half] + states[8 * b : 8 * b + 8, at : at + width].astype(F32)
        at += width
        for half in range(2):
            for k in range(width // 128):
                tile = (first + half * width) // 128 + k
                q, lane = 8 * (tile // 4), 128 * (tile % 4)
                proj_grad[q : q + 8, lane : lane + 128] = sums[half][:, 128 * k : 128 * k + 128]
    for c in copies:
        c.wait()
    val = values[...].astype(F32)
    from_start = (start_w[...] * val).astype(BF)
    to_end = (end_w[...] * val).astype(BF)
    for g in range(2):
        keys = slice(128 * g, 128 * g + 128)
        chan = slice(256 * g, 256 * g + 256)
        in_keys = in_map[:, keys]
        left = states[chan, 0:128]
        right = states[chan, 128:256]
        total = value_part[:, chan] + start_w[:, chan] * mm(in_keys, left, NT)
        total = total + end_w[:, chan] * mm(in_keys, right, NT)
        value_grad[:, chan] = total.astype(BF)
        total = in_part[:, keys] + mm(from_start[:, chan], left, NN)
        total = total + mm(to_end[:, chan], right, NN)
        in_grad[:, keys] = total.astype(BF)


def far(*args):
    far_out = (shape((TOK, CHAN)), shape((TOK, KEYS)), shape((32, CHAN), F32))
    spec = pl.GridSpec(
        grid=(1,),
        in_specs=[whole((MAIN, 256 + 1024))] + [pl.BlockSpec(memory_space=pltpu.HBM)] * 6,
        out_specs=[whole(o.shape) for o in far_out],
        scratch_shapes=[
            pltpu.VMEM((TOK, CHAN), BF),
            pltpu.VMEM((TOK, KEYS), BF),
            pltpu.VMEM((TOK, CHAN), F32),
            pltpu.VMEM((TOK, CHAN), F32),
            pltpu.VMEM((TOK, CHAN), F32),
            pltpu.VMEM((TOK, KEYS), F32),
            pltpu.SemaphoreType.DMA((6,)),
        ],
    )
    return call(far_body, far_out, 200_000_000, hbm_in=range(1, 7), grid_spec=spec)(*args)


def swap(rows):
    lanes = rows.shape[1]
    out = lax.all_to_all(rows.reshape(BLOCKS, -1, lanes), SP, 0, 0, tiled=True)
    return out.reshape(-1, lanes)


def other_core(array):
    return lax.ppermute(array, "tp", [(0, 1), (1, 0)])


def on_device(
    stream_rows,
    out_cotangent,
    expert_ids,
    route_weights,
    gate_weight,
    up_weight,
    down_weight,
    proj_weight,
    gate_input,
    scan_out,
    values,
    in_map,
    out_map,
    log_decay,
):
    tp = lax.axis_index("tp").astype(jnp.int32).reshape(1)
    ids = expert_ids.T
    sent = pack(tp, ids, route_weights.T, stream_rows, out_cotangent)
    own = swap(sent)
    x_payload, start_w, end_w, cum, cum_t = decay(values, in_map, log_decay.T)
    peer = other_core(own)
    rows_o, cot_o, *pre = expert_own(tp, own, gate_weight, up_weight, down_weight)
    rows_p, cot_p, active, pre_grad, up_grad, part_peer = expert_peer(
        tp, peer, gate_weight, up_weight, down_weight, *pre
    )
    part_in = other_core(part_peer)
    part_own = own_rows(tp, pre_grad, up_grad, gate_weight, up_weight)
    sent_back = reply(part_own, part_in, x_payload)
    back = swap(sent_back)
    gate_w_grad, up_w_grad, down_grad = weight_grads(
        tp, rows_o, cot_o, rows_p, cot_p, active, pre_grad, up_grad
    )
    stream_grad, x_states, decays = join(tp, back, ids, out_cotangent)
    stream = lax.all_gather(stream_grad, "tp")
    gate_grad, scan_grad, gated, payload = mix(
        stream, proj_weight, gate_input, scan_out, start_w, end_w, out_map, x_states
    )
    got = swap(payload)
    odd = jnp.stack([lax.axis_index(name) & 1 for name in SP]).astype(jnp.int32)
    keep, *halves = proj_part(odd, stream, gated)
    pair = [(0, 1), (1, 0), (2, 3), (3, 2)]
    others = [lax.ppermute(h, name, pair) for h, name in zip(halves, SP)]
    buffer = scan_grads(got, decays, keep, others)
    g_states = swap(buffer)
    out_grad, value_part, in_part = near(
        scan_grad, values, in_map, out_map, cum, cum_t, start_w, end_w, got[:, 256:]
    )
    value_grad, in_grad, proj_grad = far(
        g_states, values, in_map, start_w, end_w, value_part, in_part
    )
    return (
        stream_grad,
        proj_grad,
        value_grad,
        in_grad,
        out_grad,
        gate_grad,
        gate_w_grad,
        up_w_grad,
        down_grad,
    )


def solution(mesh):
    finer = Mesh(mesh.devices.reshape(4, 4, 4, mesh.shape["tp"]), ("sp_0", "sp_1", "sp_2", "tp"))
    return jax.shard_map(
        on_device,
        mesh=finer,
        in_specs=(
            P(SP, None),
            P(SP, None),
            P(SP, None),
            P(SP, None),
            P(SP, None, "tp"),
            P(SP, None, "tp"),
            P(SP, "tp", None),
            P("tp", None),
            P(SP, "tp"),
            P(SP, "tp"),
            P(SP, "tp"),
            P(SP, "tp"),
            P(SP, "tp"),
            P(SP, "tp"),
        ),
        out_specs=(
            P(SP, "tp"),
            P(SP, "tp"),
            P(SP, "tp"),
            P(SP, "tp"),
            P(SP, "tp"),
            P(SP, "tp"),
            P(SP, None, "tp"),
            P(SP, None, "tp"),
            P(SP, "tp", None),
        ),
        check_vma=False,
    )
```

```python
import jax
import jax.numpy as jnp
from jax import lax
from jax.experimental import pallas as pl
from jax.experimental.pallas import tpu as pltpu
from jax.sharding import Mesh
from jax.sharding import PartitionSpec as P


SP = ("sp_0", "sp_1", "sp_2")
ALL = SP + ("tp",)
TOK = 192
WIDTH = 2048
HALF = 1024
EXPERTS = 64
MAIN = 512
SLOTS = 576
FF = 768
FF_STEP = 256
CHAN = 512
KEYS = 256
HEADS = 8
BLOCKS = 64

BF = jnp.bfloat16
F32 = jnp.float32
EXACT = lax.Precision.HIGHEST


def mm(a, b, dims, precision=None):
    return lax.dot_general(a, b, (dims, ((), ())), preferred_element_type=F32, precision=precision)


NN = ((1,), (0,))
NT = ((1,), (1,))
TN = ((0,), (0,))


def iota(shape, dim):
    return lax.broadcasted_iota(jnp.int32, shape, dim)


def ones_where(mask):
    return jnp.where(mask, 1.0, 0.0).astype(BF)


def call(body, out_shape, flops, hbm_in=(), **kw):
    vmem = kw.pop("vmem", 12 << 20)
    kernel = pl.pallas_call(
        body,
        out_shape=out_shape,
        compiler_params=pltpu.CompilerParams(vmem_limit_bytes=vmem),
        cost_estimate=pl.CostEstimate(flops=flops, bytes_accessed=1 << 20, transcendentals=0),
        **kw,
    )

    def run(*args):
        return kernel(
            *[
                pltpu.with_memory_space_constraint(a, pltpu.HBM) if i in hbm_in else a
                for i, a in enumerate(args)
            ]
        )

    return run


def shape(dims, dtype=BF):
    return jax.ShapeDtypeStruct(dims, dtype)


def slot_choices(ids):
    expert = iota((EXPERTS, TOK), 0)
    named = [ids[k : k + 1] == expert for k in range(2)]
    either = ones_where(named[0] | named[1])
    earlier = ones_where(iota((TOK, TOK), 0) < iota((TOK, TOK), 1))
    count = mm(either, earlier, NN)
    picks = []
    for k in range(2):
        rank = jnp.sum(jnp.where(named[k], count, 0.0), axis=0, keepdims=True).astype(jnp.int32)
        own = ids[k : k + 1]
        row = jnp.where(rank < 8, own * 8 + rank, MAIN + own)
        picks.append(row == iota((SLOTS, TOK), 0))
    return picks


def fold_last(rows):
    q = iota((MAIN, MAIN), 0)
    order = ones_where(iota((MAIN, MAIN), 1) == (q & 7) * EXPERTS + (q >> 3))
    stacked = jnp.concatenate([rows[:, 128 * j : 128 * j + 128] for j in range(8)], axis=0)
    return mm(order, stacked, NN).astype(BF)


def unfold_last(folded):
    c = iota((MAIN, MAIN), 0)
    order = ones_where(iota((MAIN, MAIN), 1) == (c & 63) * 8 + (c >> 6))
    stacked = mm(order, folded, NN).astype(BF)
    return [
        jnp.concatenate(
            [stacked[64 * j : 64 * j + 64, 128 * i : 128 * i + 128] for j in range(8)], axis=1
        )
        for i in range(folded.shape[1] // 128)
    ]


def pack_body(tp, ids, weights, rows_hbm, cot_hbm, out_hbm, rows, cot, out, sems):
    at = pl.ds(pl.multiple_of(tp[0] * HALF, HALF), HALF)
    get_rows = pltpu.make_async_copy(rows_hbm.at[:, at], rows, sems.at[0])
    get_cot = pltpu.make_async_copy(cot_hbm.at[:, at], cot, sems.at[1])
    get_rows.start()
    get_cot.start()
    first, second = slot_choices(ids[...])
    both = ones_where(first | second)
    scale = jnp.where(first, weights[0:1], jnp.where(second, weights[1:2], 0.0))
    scale = jnp.sum(scale, axis=1, keepdims=True)

    def leave(k, low, high):
        lanes = slice(low, high)
        return pltpu.make_async_copy(out.at[:, lanes], out_hbm.at[:, lanes], sems.at[k])

    pieces = (leave(2, 0, HALF), leave(3, HALF, 2 * HALF), leave(4, 2 * HALF, 2 * HALF + 256))
    get_rows.wait()
    row_slots = mm(both, rows[...], NN).astype(BF)
    out[:, 0:HALF] = row_slots[:MAIN]
    pieces[0].start()
    out[:, 2 * HALF : 2 * HALF + 128] = fold_last(row_slots[MAIN:])
    get_cot.wait()
    cot_slots = (scale * mm(both, cot[...], NN)).astype(BF)
    out[:, 2 * HALF + 128 :] = fold_last(cot_slots[MAIN:])
    pieces[2].start()
    out[:, HALF : 2 * HALF] = cot_slots[:MAIN]
    pieces[1].start()
    for piece in pieces:
        piece.wait()


def whole(dims):
    return pl.BlockSpec(dims, lambda *_: (0,) * len(dims))


def pack(tp, ids, weights, rows, cot):
    spec = pltpu.PrefetchScalarGridSpec(
        num_scalar_prefetch=1,
        grid=(1,),
        in_specs=[
            whole((2, TOK)),
            whole((2, TOK)),
            pl.BlockSpec(memory_space=pltpu.HBM),
            pl.BlockSpec(memory_space=pltpu.HBM),
        ],
        out_specs=pl.BlockSpec(memory_space=pltpu.HBM),
        scratch_shapes=[
            pltpu.VMEM((TOK, HALF), BF),
            pltpu.VMEM((TOK, HALF), BF),
            pltpu.VMEM((MAIN, 2 * HALF + 256), BF),
            pltpu.SemaphoreType.DMA((5,)),
        ],
    )
    return call(
        pack_body, pltpu.HBM((MAIN, 2 * HALF + 256), BF), 1_000_000_000, hbm_in=(1, 2, 3, 4), grid_spec=spec
    )(tp, ids, weights, rows, cot)


def decay_body(values, in_map, log_decay, payload, start_w, end_w, cum_out, cum_t_out):
    upto = jnp.where(iota((TOK, TOK), 0) <= iota((TOK, TOK), 1), 1.0, 0.0)
    cum = mm(upto, log_decay[...], ((0,), (1,)), EXACT)
    cum_t = mm(log_decay[...], upto, NN, EXACT)
    cum_out[...] = cum
    cum_t_out[...] = cum_t
    spread = jnp.where(iota((HEADS, CHAN), 1) // 64 == iota((HEADS, CHAN), 0), 1.0, 0.0)
    from_start = mm(jnp.exp(cum), spread, NN, EXACT)
    to_end = mm(jnp.exp(cum[TOK - 1 :, :] - cum), spread, NN, EXACT)
    start_w[...] = from_start
    end_w[...] = to_end
    val = values[...].astype(F32)
    block_states(payload, (to_end * val).astype(BF), (from_start * val).astype(BF), in_map)
    total = jnp.exp(cum_t[:, TOK - 1 :])
    total = jnp.concatenate(
        [jnp.broadcast_to(total[h : h + 1], (64, 128)) for h in range(HEADS)], axis=0
    )
    high = total.astype(BF)
    rest = total - high.astype(F32)
    mid = rest.astype(BF)
    low = (rest - mid.astype(F32)).astype(BF)
    part = iota((MAIN, 128), 0) & 7
    parts = jnp.where(part == 0, high.astype(F32), 0.0)
    parts = jnp.where(part == 1, mid.astype(F32), parts)
    parts = jnp.where(part == 2, low.astype(F32), parts)
    payload[:, 256:] = parts.astype(BF)


def block_states(payload, to_end, from_start, keys):
    for g in range(2):
        chan = slice(256 * g, 256 * g + 256)
        key = keys[:, 128 * g : 128 * g + 128]
        payload[chan, 0:128] = mm(to_end[:, chan], key, TN).astype(BF)
        payload[chan, 128:256] = mm(from_start[:, chan], key, TN).astype(BF)


def decay(values, in_map, log_decay):
    return call(
        decay_body,
        (
            shape((MAIN, 384)),
            shape((TOK, CHAN), F32),
            shape((TOK, CHAN), F32),
            shape((TOK, HEADS), F32),
            shape((HEADS, TOK), F32),
        ),
        1_000_000_000,
    )(values, in_map, log_decay)


def silu_parts(x):
    squash = 0.5 * jnp.tanh(0.5 * x) + 0.5
    return x * squash, squash * (1.0 + x * (1.0 - squash))


def split_slots(got, rows, cot):
    rows[:MAIN] = got[:, 0:HALF]
    cot[:MAIN] = got[:, HALF : 2 * HALF]
    last_rows, last_cot = unfold_last(got[:, 2 * HALF :])
    rows[MAIN:] = last_rows
    cot[MAIN:] = last_cot


def fetch(half, gate_h, up_h, down_h, gate_w, up_w, down_w, sems):
    wide = pl.ds(pl.multiple_of(half * HALF, HALF), HALF)
    steps = []
    for j in range(FF // FF_STEP):
        part = pl.ds(j * FF_STEP, FF_STEP)
        steps.append(
            (
                pltpu.make_async_copy(gate_h.at[0, wide, part], gate_w.at[j], sems.at[j, 0]),
                pltpu.make_async_copy(up_h.at[0, wide, part], up_w.at[j], sems.at[j, 1]),
                pltpu.make_async_copy(down_h.at[0, part, wide], down_w.at[j], sems.at[j, 2]),
            )
        )
    return steps


def open_step(half, got, weights_h, rows_h, cot_h, rows, cot, weights, sems, out_sems):
    step = pl.program_id(0)
    copies = fetch(half, *weights_h, *weights, sems)
    keep = (
        pltpu.make_async_copy(rows, rows_h, out_sems.at[0]),
        pltpu.make_async_copy(cot, cot_h, out_sems.at[1]),
    )

    @pl.when(step == 0)
    def _():
        for group in copies:
            for c in group:
                c.start()
        split_slots(got, rows, cot)
        for c in keep:
            c.start()

    for j, group in enumerate(copies):

        @pl.when(step == j)
        def _():
            for c in group:
                c.wait()

    return step, keep


def own_body(
    tp, own, gate_h, up_h, down_h, rows_h, cot_h, gate_o, up_o, act_o,
    rows, cot, gate_w, up_w, down_w, sems, out_sems,
):
    step, keep = open_step(
        tp[0], own, (gate_h, up_h, down_h), rows_h, cot_h, rows, cot, (gate_w, up_w, down_w),
        sems, out_sems,
    )
    gate_o[...] = mm(rows[...], gate_w[step], NN)
    up_o[...] = mm(rows[...], up_w[step], NN)
    act_o[...] = mm(cot[...], down_w[step], NT)

    @pl.when(step == 2)
    def _():
        for c in keep:
            c.wait()


def step_block(dims):
    return pl.BlockSpec(dims, lambda i, t: (0, i))


HBM = pl.BlockSpec(memory_space=pltpu.HBM)
EXPERT_SCRATCH = [
    pltpu.VMEM((SLOTS, HALF), BF),
    pltpu.VMEM((SLOTS, HALF), BF),
    pltpu.VMEM((3, HALF, FF_STEP), BF),
    pltpu.VMEM((3, HALF, FF_STEP), BF),
    pltpu.VMEM((3, FF_STEP, HALF), BF),
    pltpu.SemaphoreType.DMA((3, 3)),
    pltpu.SemaphoreType.DMA((2,)),
]


def expert_own(tp, own, gate_w, up_w, down_w):
    spec = pltpu.PrefetchScalarGridSpec(
        num_scalar_prefetch=1,
        grid=(FF // FF_STEP,),
        in_specs=[whole((MAIN, 2 * HALF + 256)), HBM, HBM, HBM],
        out_specs=[HBM, HBM] + [step_block((SLOTS, FF_STEP))] * 3,
        scratch_shapes=EXPERT_SCRATCH,
    )
    return call(
        own_body,
        [pltpu.HBM((SLOTS, HALF), BF)] * 2 + [shape((SLOTS, FF), F32)] * 3,
        2_700_000_000,
        hbm_in=(2, 3, 4),
        grid_spec=spec,
        vmem=24 << 20,
    )(tp, own, gate_w, up_w, down_w)


def peer_body(
    tp, peer, gate_h, up_h, down_h, gate_o, up_o, act_o,
    rows_h, cot_h, active, pre_grad, up_grad, part,
    rows, cot, gate_w, up_w, down_w, sems, out_sems, acc,
):
    step, keep = open_step(
        1 - tp[0], peer, (gate_h, up_h, down_h), rows_h, cot_h, rows, cot, (gate_w, up_w, down_w),
        sems, out_sems,
    )
    for first in range(0, SLOTS, SLOTS // 2):
        at = slice(first, first + SLOTS // 2)
        gate_pre = gate_o[at] + mm(rows[at], gate_w[step], NN)
        up_val = up_o[at] + mm(rows[at], up_w[step], NN)
        act_grad = act_o[at] + mm(cot[at], down_w[step], NT)
        act, slope = silu_parts(gate_pre)
        active[at] = (act * up_val).astype(BF)
        up_grad[at] = (act_grad * act).astype(BF)
        pre_grad[at] = (act_grad * up_val * slope).astype(BF)
    for first in range(0, SLOTS, SLOTS // 2):
        at = slice(first, first + SLOTS // 2)
        before = jnp.where(step == 0, 0.0, acc[at])
        acc[at] = before + mm(pre_grad[at], gate_w[step], NT) + mm(up_grad[at], up_w[step], NT)

    @pl.when(step == 2)
    def _():
        part[...] = acc[...].astype(BF)
        for c in keep:
            c.wait()


def expert_peer(tp, peer, gate_w, up_w, down_w, gate_o, up_o, act_o):
    spec = pltpu.PrefetchScalarGridSpec(
        num_scalar_prefetch=1,
        grid=(FF // FF_STEP,),
        in_specs=[whole((MAIN, 2 * HALF + 256)), HBM, HBM, HBM]
        + [step_block((SLOTS, FF_STEP))] * 3,
        out_specs=[HBM, HBM] + [step_block((SLOTS, FF_STEP))] * 3 + [whole((SLOTS, HALF))],
        scratch_shapes=EXPERT_SCRATCH + [pltpu.VMEM((SLOTS, HALF), F32)],
    )
    return call(
        peer_body,
        [pltpu.HBM((SLOTS, HALF), BF)] * 2
        + [shape((SLOTS, FF))] * 3
        + [shape((SLOTS, HALF))],
        4_500_000_000,
        hbm_in=(2, 3, 4),
        grid_spec=spec,
        vmem=28 << 20,
    )(tp, peer, gate_w, up_w, down_w, gate_o, up_o, act_o)


def rows_body(tp, pre_grad, up_grad, gate_w, up_w, part):
    total = mm(pre_grad[...], gate_w[0], NT) + mm(up_grad[...], up_w[0], NT)
    part[...] = total.astype(BF)


def own_rows(tp, pre_grad, up_grad, gate_w, up_w):
    spec = pltpu.PrefetchScalarGridSpec(
        num_scalar_prefetch=1,
        grid=(4,),
        in_specs=[
            whole((SLOTS, FF)),
            whole((SLOTS, FF)),
            pl.BlockSpec((1, HALF // 4, FF), lambda i, t: (0, 4 * t[0] + i, 0)),
            pl.BlockSpec((1, HALF // 4, FF), lambda i, t: (0, 4 * t[0] + i, 0)),
        ],
        out_specs=step_block((SLOTS, HALF // 4)),
    )
    return call(
        rows_body, shape((SLOTS, HALF)), 1_800_000_000, grid_spec=spec, vmem=12 << 20
    )(tp, pre_grad, up_grad, gate_w, up_w)


def weight_body(tp, rows_o, cot_o, rows_p, cot_p, active, pre_grad, up_grad, gate_g, up_g, down_g):
    for half, rows, cot in ((0, rows_o, cot_o), (1, rows_p, cot_p)):

        @pl.when(pl.program_id(0) // 2 == half)
        def _():
            gate_g[0] = mm(rows[...], pre_grad[...], TN).astype(BF)
            up_g[0] = mm(rows[...], up_grad[...], TN).astype(BF)
            down_g[0] = mm(active[...], cot[...], TN).astype(BF)


def weight_grads(tp, rows_o, cot_o, rows_p, cot_p, active, pre_grad, up_grad):
    quarter = HALF // 2

    def block(i, t):
        return (t[0] * (1 - i // 2) + (1 - t[0]) * (i // 2)) * 2 + i % 2

    spec = pltpu.PrefetchScalarGridSpec(
        num_scalar_prefetch=1,
        grid=(4,),
        in_specs=[pl.BlockSpec((SLOTS, quarter), lambda i, t: (0, i % 2))] * 4
        + [whole((SLOTS, FF))] * 3,
        out_specs=[
            pl.BlockSpec((1, quarter, FF), lambda i, t: (0, block(i, t), 0)),
            pl.BlockSpec((1, quarter, FF), lambda i, t: (0, block(i, t), 0)),
            pl.BlockSpec((1, FF, quarter), lambda i, t: (0, 0, block(i, t))),
        ],
    )
    return call(
        weight_body,
        (shape((1, WIDTH, FF)), shape((1, WIDTH, FF)), shape((1, FF, WIDTH))),
        5_400_000_000,
        hbm_in=(1, 2, 3, 4),
        grid_spec=spec,
        vmem=24 << 20,
    )(tp, rows_o, cot_o, rows_p, cot_p, active, pre_grad, up_grad)


def reply_body(own, peer, states, out):
    total = (own[...].astype(F32) + peer[...].astype(F32)).astype(BF)
    out[:, 0:HALF] = total[:MAIN]
    out[:, HALF : HALF + 128] = fold_last(total[MAIN:])
    out[:, HALF + 128 :] = states[...]


def reply(own, peer, states):
    return call(reply_body, shape((MAIN, HALF + 128 + 384)), 100_000_000)(own, peer, states)


def scan_states(left_in, right_in, decays, out, work):
    def factor(b):
        at = 8 * b
        return decays[at : at + 1] + decays[at + 1 : at + 2] + decays[at + 2 : at + 3]

    factors = [factor(b) for b in range(BLOCKS)]
    left = jnp.zeros((8, 128), F32)
    right = jnp.zeros((8, 128), F32)
    for b in range(BLOCKS):
        at = 8 * b
        work[at : at + 8, 0:128] = left
        left = factors[b] * left + left_in[at : at + 8]
        back = BLOCKS - 1 - b
        at = 8 * back
        work[at : at + 8, 128:256] = right
        right = factors[back] * right + right_in[at : at + 8]
    out[:, 0:256] = work[...].astype(BF)


def join_body(tp, got, ids, cot, out, states, decays, work, wide):
    first, second = slot_choices(ids[...])
    both = ones_where(first | second)
    (last,) = unfold_last(got[:, HALF : HALF + 128])
    total = mm(both[:MAIN], got[:, :HALF], TN) + mm(both[MAIN:], last, TN)
    out[...] = (cot[...].astype(F32) + total).astype(BF)
    wide[...] = got[:, HALF + 128 :].astype(F32)
    decays[...] = wide[:, 256:]
    scan_states(wide[:, 0:128], wide[:, 128:256], wide[:, 256:], states, work)


def join(tp, got, ids, cot):
    spec = pltpu.PrefetchScalarGridSpec(
        num_scalar_prefetch=1,
        grid=(1,),
        in_specs=[
            whole((MAIN, HALF + 512)),
            whole((2, TOK)),
            pl.BlockSpec((TOK, HALF), lambda i, t: (0, t[0])),
        ],
        out_specs=[whole((TOK, HALF)), whole((MAIN, 256)), whole((MAIN, 128))],
        scratch_shapes=[pltpu.VMEM((MAIN, 256), F32), pltpu.VMEM((MAIN, 384), F32)],
    )
    return call(
        join_body,
        (shape((TOK, HALF)), shape((MAIN, 256)), shape((MAIN, 128), F32)),
        300_000_000,
        grid_spec=spec,
    )(tp, got, ids, cot)


def mix_body(
    stream, proj_w, gate_in, scan_out, start_w, end_w, out_map, x_states,
    gate_grad, scan_grad, gated, payload,
):
    mixed = mm(stream[0], proj_w[:, :HALF], NT) + mm(stream[1], proj_w[:, HALF:], NT)
    scan = scan_out[...].astype(F32)
    act, slope = silu_parts(gate_in[...].astype(F32))
    gated[...] = (scan * act).astype(BF)
    gate_grad[...] = (mixed * scan * slope).astype(BF)
    grad = (mixed * act).astype(BF)
    scan_grad[...] = grad
    wide = grad.astype(F32)
    block_states(
        payload, (end_w[...] * wide).astype(BF), (start_w[...] * wide).astype(BF), out_map
    )
    payload[:, 256:] = x_states[...]


def mix(*args):
    return call(
        mix_body,
        (shape((TOK, CHAN)), shape((TOK, CHAN)), shape((TOK, CHAN)), shape((MAIN, 512))),
        500_000_000,
    )(*args)


PARTS = ((0, 640), (1280, 384))


def proj_body(odd, stream, gated, keep, *sends):
    for i in range(2):
        part = mm(stream[i], gated[...], TN).reshape(32, 4, 8, CHAN)
        flat = [part[:, q].reshape(256, CHAN) for q in range(4)]
        rows = slice(256 * i, 256 * i + 256)

        def tile(t):
            return flat[t // 4][:, 128 * (t % 4) : 128 * (t % 4) + 128]

        at = 0
        for j, (first, width) in enumerate(PARTS):
            for k in range(width // 128):
                low = tile(first // 128 + k)
                high = tile((first + width) // 128 + k)
                upper = odd[j] == 1
                keep[rows, at : at + 128] = jnp.where(upper, high, low).astype(BF)
                sends[j][rows, 128 * k : 128 * k + 128] = jnp.where(upper, low, high).astype(BF)
                at += 128


def proj_part(odd, stream, gated):
    out = [pltpu.HBM((MAIN, 1024), BF)] + [shape((MAIN, width)) for _, width in PARTS]
    spec = pltpu.PrefetchScalarGridSpec(
        num_scalar_prefetch=1,
        grid=(1,),
        in_specs=[whole((2, TOK, HALF)), whole((TOK, CHAN))],
        out_specs=[whole(o.shape) for o in out],
    )
    return call(proj_body, out, 400_000_000, grid_spec=spec)(odd, stream, gated)


def scan_body(got, decays, keep_h, first, second, out, work, wide, keep, sem):
    fetch_keep = pltpu.make_async_copy(keep_h, keep, sem.at[0])
    fetch_keep.start()
    wide[...] = got[:, 0:256].astype(F32)
    scan_states(wide[:, 0:128], wide[:, 128:256], decays[...], out, work)
    fetch_keep.wait()
    at = 0
    for other in (first, second):
        width = other.shape[1]
        total = keep[:, at : at + width].astype(F32) + other[...].astype(F32)
        out[:, 256 + at : 256 + at + width] = total.astype(BF)
        at += width


def scan_grads(got, decays, keep, others):
    spec = pl.GridSpec(
        grid=(1,),
        in_specs=[whole((MAIN, 512)), whole((MAIN, 128)), HBM] + [whole(o.shape) for o in others],
        out_specs=whole((MAIN, 256 + 1024)),
        scratch_shapes=[
            pltpu.VMEM((MAIN, 256), F32),
            pltpu.VMEM((MAIN, 256), F32),
            pltpu.VMEM((MAIN, 1024), BF),
            pltpu.SemaphoreType.DMA((1,)),
        ],
    )
    return call(
        scan_body, shape((MAIN, 256 + 1024)), 100_000_000, hbm_in=(2,), grid_spec=spec
    )(got, decays, keep, *others)


def near_body(
    scan_grad, values, in_map, out_map, cum, cum_t, start_w, end_w, states,
    out_grad, value_part, in_part,
):
    wide = scan_grad[...].astype(F32)
    from_start = (start_w[...] * wide).astype(BF)
    to_end = (end_w[...] * wide).astype(BF)
    for g in range(2):
        keys = slice(128 * g, 128 * g + 128)
        chan = slice(256 * g, 256 * g + 256)
        in_keys = in_map[:, keys]
        out_keys = out_map[:, keys]
        meet = mm(out_keys, in_keys, NT)
        pair_sum = jnp.zeros((TOK, TOK), F32)
        for e in range(4):
            h = 4 * g + e
            at = slice(64 * h, 64 * h + 64)
            kernel = jnp.exp(-jnp.abs(cum[:, h : h + 1] - cum_t[h : h + 1, :]))
            grad = scan_grad[:, at]
            value_part[:, at] = mm((kernel * meet).astype(BF), grad, TN)
            pair_sum = pair_sum + kernel * mm(grad, values[:, at], NT)
        pair_sum = pair_sum.astype(BF)
        out_total = mm(pair_sum, in_keys, NN)
        out_total = out_total + mm(from_start[:, chan], states[chan, 0:128], NN)
        out_total = out_total + mm(to_end[:, chan], states[chan, 128:256], NN)
        out_grad[:, keys] = out_total.astype(BF)
        in_part[:, keys] = mm(pair_sum, out_keys, TN)


def near(*args):
    return call(
        near_body,
        (shape((TOK, KEYS)), shape((TOK, CHAN), F32), shape((TOK, KEYS), F32)),
        600_000_000,
    )(*args)


def far_body(
    tp, states, values_h, in_map_h, start_h, end_h, value_part_h, in_part_h,
    value_grad, in_grad, proj_grad,
    values, in_map, start_w, end_w, value_part, in_part, sems,
):
    pairs = (
        (values_h, values),
        (in_map_h, in_map),
        (start_h, start_w),
        (end_h, end_w),
        (value_part_h, value_part),
        (in_part_h, in_part),
    )
    copies = [pltpu.make_async_copy(a, b, sems.at[i]) for i, (a, b) in enumerate(pairs)]
    for c in copies:
        c.start()
    at = 256
    for j, (first, width) in enumerate(PARTS):
        sums = [[jnp.zeros((8, width), F32) for _ in range(2)] for _ in range(2)]
        for b in range(BLOCKS):
            chunk = states[8 * b : 8 * b + 8, at : at + width].astype(F32)
            here = sums[(b >> 4) & 1] if j == 0 else sums[b & 1]
            other = (b >> 2) & 1
            here[other] = here[other] + chunk
        at += width
        for half in range(2):
            total = sums[half][0] + sums[half][1]
            if j == 0:
                total = jnp.where(tp[0] == 0, total, sums[0][half] + sums[1][half])
            for k in range(width // 128):
                tile = (first + half * width) // 128 + k
                q, lane = 8 * (tile // 4), 128 * (tile % 4)
                proj_grad[q : q + 8, lane : lane + 128] = total[:, 128 * k : 128 * k + 128]
    for c in copies:
        c.wait()
    val = values[...].astype(F32)
    from_start = (start_w[...] * val).astype(BF)
    to_end = (end_w[...] * val).astype(BF)
    for g in range(2):
        keys = slice(128 * g, 128 * g + 128)
        chan = slice(256 * g, 256 * g + 256)
        in_keys = in_map[:, keys]
        left = states[chan, 0:128]
        right = states[chan, 128:256]
        total = value_part[:, chan] + start_w[:, chan] * mm(in_keys, left, NT)
        total = total + end_w[:, chan] * mm(in_keys, right, NT)
        value_grad[:, chan] = total.astype(BF)
        total = in_part[:, keys] + mm(from_start[:, chan], left, NN)
        total = total + mm(to_end[:, chan], right, NN)
        in_grad[:, keys] = total.astype(BF)


def far(*args):
    far_out = (shape((TOK, CHAN)), shape((TOK, KEYS)), shape((32, CHAN), F32))
    spec = pltpu.PrefetchScalarGridSpec(
        num_scalar_prefetch=1,
        grid=(1,),
        in_specs=[whole((MAIN, 256 + 1024))] + [pl.BlockSpec(memory_space=pltpu.HBM)] * 6,
        out_specs=[whole(o.shape) for o in far_out],
        scratch_shapes=[
            pltpu.VMEM((TOK, CHAN), BF),
            pltpu.VMEM((TOK, KEYS), BF),
            pltpu.VMEM((TOK, CHAN), F32),
            pltpu.VMEM((TOK, CHAN), F32),
            pltpu.VMEM((TOK, CHAN), F32),
            pltpu.VMEM((TOK, KEYS), F32),
            pltpu.SemaphoreType.DMA((6,)),
        ],
    )
    return call(far_body, far_out, 200_000_000, hbm_in=range(2, 8), grid_spec=spec)(*args)


def swap(rows):
    lanes = rows.shape[1]
    out = lax.all_to_all(rows.reshape(BLOCKS, -1, lanes), SP, 0, 0, tiled=True)
    return out.reshape(-1, lanes)


def pairs_of(piece):
    out = []
    for source in range(128):
        step = 2 if piece else 32 if source % 2 == 0 else 8
        out.append((source, source ^ step))
    return out


def other_core(array):
    return lax.ppermute(array, "tp", [(0, 1), (1, 0)])


def on_device(
    stream_rows,
    out_cotangent,
    expert_ids,
    route_weights,
    gate_weight,
    up_weight,
    down_weight,
    proj_weight,
    gate_input,
    scan_out,
    values,
    in_map,
    out_map,
    log_decay,
):
    tp = lax.axis_index("tp").astype(jnp.int32).reshape(1)
    ids = expert_ids.T
    sent = pack(tp, ids, route_weights.T, stream_rows, out_cotangent)
    own = swap(sent)
    x_payload, start_w, end_w, cum, cum_t = decay(values, in_map, log_decay.T)
    peer = other_core(own)
    rows_o, cot_o, *pre = expert_own(tp, own, gate_weight, up_weight, down_weight)
    rows_p, cot_p, active, pre_grad, up_grad, part_peer = expert_peer(
        tp, peer, gate_weight, up_weight, down_weight, *pre
    )
    part_in = other_core(part_peer)
    part_own = own_rows(tp, pre_grad, up_grad, gate_weight, up_weight)
    sent_back = reply(part_own, part_in, x_payload)
    back = swap(sent_back)
    gate_w_grad, up_w_grad, down_grad = weight_grads(
        tp, rows_o, cot_o, rows_p, cot_p, active, pre_grad, up_grad
    )
    stream_grad, x_states, decays = join(tp, back, ids, out_cotangent)
    stream = lax.all_gather(stream_grad, "tp")
    gate_grad, scan_grad, gated, payload = mix(
        stream, proj_weight, gate_input, scan_out, start_w, end_w, out_map, x_states
    )
    got = swap(payload)
    place = [lax.axis_index(name).astype(jnp.int32) & 1 for name in SP]
    odd = jnp.stack([jnp.where(tp[0] == 0, place[0], place[1]), place[2]])
    keep, *halves = proj_part(odd, stream, gated)
    others = [lax.ppermute(h, ALL, pairs_of(i)) for i, h in enumerate(halves)]
    buffer = scan_grads(got, decays, keep, others)
    g_states = swap(buffer)
    out_grad, value_part, in_part = near(
        scan_grad, values, in_map, out_map, cum, cum_t, start_w, end_w, got[:, 256:]
    )
    value_grad, in_grad, proj_grad = far(
        tp, g_states, values, in_map, start_w, end_w, value_part, in_part
    )
    return (
        stream_grad,
        proj_grad,
        value_grad,
        in_grad,
        out_grad,
        gate_grad,
        gate_w_grad,
        up_w_grad,
        down_grad,
    )


def solution(mesh):
    finer = Mesh(mesh.devices.reshape(4, 4, 4, mesh.shape["tp"]), ("sp_0", "sp_1", "sp_2", "tp"))
    return jax.shard_map(
        on_device,
        mesh=finer,
        in_specs=(
            P(SP, None),
            P(SP, None),
            P(SP, None),
            P(SP, None),
            P(SP, None, "tp"),
            P(SP, None, "tp"),
            P(SP, "tp", None),
            P("tp", None),
            P(SP, "tp"),
            P(SP, "tp"),
            P(SP, "tp"),
            P(SP, "tp"),
            P(SP, "tp"),
            P(SP, "tp"),
        ),
        out_specs=(
            P(SP, "tp"),
            P(SP, "tp"),
            P(SP, "tp"),
            P(SP, "tp"),
            P(SP, "tp"),
            P(SP, "tp"),
            P(SP, None, "tp"),
            P(SP, None, "tp"),
            P(SP, "tp", None),
        ),
        check_vma=False,
    )
```

```python
import jax
import jax.numpy as jnp
from jax import lax
from jax.experimental import pallas as pl
from jax.experimental.pallas import tpu as pltpu
from jax.sharding import Mesh
from jax.sharding import PartitionSpec as P


SP = ("sp_0", "sp_1", "sp_2")
ALL = SP + ("tp",)
TOK = 192
WIDTH = 2048
HALF = 1024
EXPERTS = 64
MAIN = 512
SLOTS = 576
FF = 768
FF_STEP = 256
CHAN = 512
KEYS = 256
HEADS = 8
BLOCKS = 64

BF = jnp.bfloat16
F32 = jnp.float32
EXACT = lax.Precision.HIGHEST


def mm(a, b, dims, precision=None):
    return lax.dot_general(a, b, (dims, ((), ())), preferred_element_type=F32, precision=precision)


NN = ((1,), (0,))
NT = ((1,), (1,))
TN = ((0,), (0,))


def iota(shape, dim):
    return lax.broadcasted_iota(jnp.int32, shape, dim)


def ones_where(mask):
    return jnp.where(mask, 1.0, 0.0).astype(BF)


def call(body, out_shape, flops, hbm_in=(), **kw):
    vmem = kw.pop("vmem", 12 << 20)
    kernel = pl.pallas_call(
        body,
        out_shape=out_shape,
        compiler_params=pltpu.CompilerParams(vmem_limit_bytes=vmem),
        cost_estimate=pl.CostEstimate(flops=flops, bytes_accessed=1 << 20, transcendentals=0),
        **kw,
    )

    def run(*args):
        return kernel(
            *[
                pltpu.with_memory_space_constraint(a, pltpu.HBM) if i in hbm_in else a
                for i, a in enumerate(args)
            ]
        )

    return run


def shape(dims, dtype=BF):
    return jax.ShapeDtypeStruct(dims, dtype)


def slot_choices(ids):
    expert = iota((EXPERTS, TOK), 0)
    named = [ids[k : k + 1] == expert for k in range(2)]
    either = ones_where(named[0] | named[1])
    earlier = ones_where(iota((TOK, TOK), 0) < iota((TOK, TOK), 1))
    count = mm(either, earlier, NN)
    picks = []
    for k in range(2):
        rank = jnp.sum(jnp.where(named[k], count, 0.0), axis=0, keepdims=True).astype(jnp.int32)
        own = ids[k : k + 1]
        row = jnp.where(rank < 8, own * 8 + rank, MAIN + own)
        picks.append(row == iota((SLOTS, TOK), 0))
    return picks


def fold_last(rows):
    q = iota((MAIN, MAIN), 0)
    order = ones_where(iota((MAIN, MAIN), 1) == (q & 7) * EXPERTS + (q >> 3))
    stacked = jnp.concatenate([rows[:, 128 * j : 128 * j + 128] for j in range(8)], axis=0)
    return mm(order, stacked, NN).astype(BF)


def unfold_last(folded):
    c = iota((MAIN, MAIN), 0)
    order = ones_where(iota((MAIN, MAIN), 1) == (c & 63) * 8 + (c >> 6))
    stacked = mm(order, folded, NN).astype(BF)
    return [
        jnp.concatenate(
            [stacked[64 * j : 64 * j + 64, 128 * i : 128 * i + 128] for j in range(8)], axis=1
        )
        for i in range(folded.shape[1] // 128)
    ]


def pack_body(tp, ids, weights, rows_hbm, cot_hbm, out_hbm, rows, cot, out, sems):
    at = pl.ds(pl.multiple_of(tp[0] * HALF, HALF), HALF)
    get_rows = pltpu.make_async_copy(rows_hbm.at[:, at], rows, sems.at[0])
    get_cot = pltpu.make_async_copy(cot_hbm.at[:, at], cot, sems.at[1])
    get_rows.start()
    get_cot.start()
    first, second = slot_choices(ids[...])
    both = ones_where(first | second)
    scale = jnp.where(first, weights[0:1], jnp.where(second, weights[1:2], 0.0))
    scale = jnp.sum(scale, axis=1, keepdims=True)

    def leave(k, low, high):
        lanes = slice(low, high)
        return pltpu.make_async_copy(out.at[:, lanes], out_hbm.at[:, lanes], sems.at[k])

    pieces = (leave(2, 0, HALF), leave(3, HALF, 2 * HALF), leave(4, 2 * HALF, 2 * HALF + 256))
    get_rows.wait()
    row_slots = mm(both, rows[...], NN).astype(BF)
    out[:, 0:HALF] = row_slots[:MAIN]
    pieces[0].start()
    out[:, 2 * HALF : 2 * HALF + 128] = fold_last(row_slots[MAIN:])
    get_cot.wait()
    cot_slots = (scale * mm(both, cot[...], NN)).astype(BF)
    out[:, 2 * HALF + 128 :] = fold_last(cot_slots[MAIN:])
    pieces[2].start()
    out[:, HALF : 2 * HALF] = cot_slots[:MAIN]
    pieces[1].start()
    for piece in pieces:
        piece.wait()


def whole(dims):
    return pl.BlockSpec(dims, lambda *_: (0,) * len(dims))


def pack(tp, ids, weights, rows, cot):
    spec = pltpu.PrefetchScalarGridSpec(
        num_scalar_prefetch=1,
        grid=(1,),
        in_specs=[
            whole((2, TOK)),
            whole((2, TOK)),
            pl.BlockSpec(memory_space=pltpu.HBM),
            pl.BlockSpec(memory_space=pltpu.HBM),
        ],
        out_specs=pl.BlockSpec(memory_space=pltpu.HBM),
        scratch_shapes=[
            pltpu.VMEM((TOK, HALF), BF),
            pltpu.VMEM((TOK, HALF), BF),
            pltpu.VMEM((MAIN, 2 * HALF + 256), BF),
            pltpu.SemaphoreType.DMA((5,)),
        ],
    )
    return call(
        pack_body, pltpu.HBM((MAIN, 2 * HALF + 256), BF), 1_000_000_000, hbm_in=(1, 2, 3, 4), grid_spec=spec
    )(tp, ids, weights, rows, cot)


def decay_body(values, in_map, log_decay, payload, start_w, end_w, cum_out, cum_t_out):
    upto = jnp.where(iota((TOK, TOK), 0) <= iota((TOK, TOK), 1), 1.0, 0.0)
    cum = mm(upto, log_decay[...], ((0,), (1,)), EXACT)
    cum_t = mm(log_decay[...], upto, NN, EXACT)
    cum_out[...] = cum
    cum_t_out[...] = cum_t
    spread = jnp.where(iota((HEADS, CHAN), 1) // 64 == iota((HEADS, CHAN), 0), 1.0, 0.0)
    from_start = mm(jnp.exp(cum), spread, NN, EXACT)
    to_end = mm(jnp.exp(cum[TOK - 1 :, :] - cum), spread, NN, EXACT)
    start_w[...] = from_start
    end_w[...] = to_end
    val = values[...].astype(F32)
    block_states(payload, (to_end * val).astype(BF), (from_start * val).astype(BF), in_map)
    total = jnp.exp(cum_t[:, TOK - 1 :])
    total = jnp.concatenate(
        [jnp.broadcast_to(total[h : h + 1], (64, 128)) for h in range(HEADS)], axis=0
    )
    high = total.astype(BF)
    rest = total - high.astype(F32)
    mid = rest.astype(BF)
    low = (rest - mid.astype(F32)).astype(BF)
    part = iota((MAIN, 128), 0) & 7
    parts = jnp.where(part == 0, high.astype(F32), 0.0)
    parts = jnp.where(part == 1, mid.astype(F32), parts)
    parts = jnp.where(part == 2, low.astype(F32), parts)
    payload[:, 256:] = parts.astype(BF)


def block_states(payload, to_end, from_start, keys):
    for g in range(2):
        chan = slice(256 * g, 256 * g + 256)
        key = keys[:, 128 * g : 128 * g + 128]
        payload[chan, 0:128] = mm(to_end[:, chan], key, TN).astype(BF)
        payload[chan, 128:256] = mm(from_start[:, chan], key, TN).astype(BF)


def decay(values, in_map, log_decay):
    return call(
        decay_body,
        (
            shape((MAIN, 384)),
            shape((TOK, CHAN), F32),
            shape((TOK, CHAN), F32),
            shape((TOK, HEADS), F32),
            shape((HEADS, TOK), F32),
        ),
        1_000_000_000,
    )(values, in_map, log_decay)


def silu_parts(x):
    squash = 0.5 * jnp.tanh(0.5 * x) + 0.5
    return x * squash, squash * (1.0 + x * (1.0 - squash))


def split_slots(got, rows, cot):
    rows[:MAIN] = got[:, 0:HALF]
    cot[:MAIN] = got[:, HALF : 2 * HALF]
    last_rows, last_cot = unfold_last(got[:, 2 * HALF :])
    rows[MAIN:] = last_rows
    cot[MAIN:] = last_cot


def fetch(half, gate_h, up_h, down_h, gate_w, up_w, down_w, sems):
    wide = pl.ds(pl.multiple_of(half * HALF, HALF), HALF)
    steps = []
    for j in range(FF // FF_STEP):
        part = pl.ds(j * FF_STEP, FF_STEP)
        steps.append(
            (
                pltpu.make_async_copy(gate_h.at[0, wide, part], gate_w.at[j], sems.at[j, 0]),
                pltpu.make_async_copy(up_h.at[0, wide, part], up_w.at[j], sems.at[j, 1]),
                pltpu.make_async_copy(down_h.at[0, part, wide], down_w.at[j], sems.at[j, 2]),
            )
        )
    return steps


def open_step(half, got, weights_h, rows_h, cot_h, rows, cot, weights, sems, out_sems):
    step = pl.program_id(0)
    copies = fetch(half, *weights_h, *weights, sems)
    keep = (
        pltpu.make_async_copy(rows, rows_h, out_sems.at[0]),
        pltpu.make_async_copy(cot, cot_h, out_sems.at[1]),
    )

    def start(group):
        for c in group:
            c.start()

    @pl.when(step == 0)
    def _():
        start(copies[0])
        split_slots(got, rows, cot)

    for j, group in enumerate(copies):

        @pl.when(step == j)
        def _():
            for c in group:
                c.wait()
            if j == 0:
                start(copies[1])
            if j == 1:
                start(keep)
            if j < 1:
                start(copies[2])

    return step, keep


def own_body(
    tp, own, gate_h, up_h, down_h, rows_h, cot_h, gate_o, up_o, act_o,
    rows, cot, gate_w, up_w, down_w, sems, out_sems,
):
    step, keep = open_step(
        tp[0], own, (gate_h, up_h, down_h), rows_h, cot_h, rows, cot, (gate_w, up_w, down_w),
        sems, out_sems,
    )
    gate_o[...] = mm(rows[...], gate_w[step], NN)
    up_o[...] = mm(rows[...], up_w[step], NN)
    act_o[...] = mm(cot[...], down_w[step], NT)

    @pl.when(step == 2)
    def _():
        for c in keep:
            c.wait()


def step_block(dims):
    return pl.BlockSpec(dims, lambda i, t: (0, i))


HBM = pl.BlockSpec(memory_space=pltpu.HBM)
EXPERT_SCRATCH = [
    pltpu.VMEM((SLOTS, HALF), BF),
    pltpu.VMEM((SLOTS, HALF), BF),
    pltpu.VMEM((3, HALF, FF_STEP), BF),
    pltpu.VMEM((3, HALF, FF_STEP), BF),
    pltpu.VMEM((3, FF_STEP, HALF), BF),
    pltpu.SemaphoreType.DMA((3, 3)),
    pltpu.SemaphoreType.DMA((2,)),
]


def expert_own(tp, own, gate_w, up_w, down_w):
    spec = pltpu.PrefetchScalarGridSpec(
        num_scalar_prefetch=1,
        grid=(FF // FF_STEP,),
        in_specs=[whole((MAIN, 2 * HALF + 256)), HBM, HBM, HBM],
        out_specs=[HBM, HBM] + [step_block((SLOTS, FF_STEP))] * 3,
        scratch_shapes=EXPERT_SCRATCH,
    )
    return call(
        own_body,
        [pltpu.HBM((SLOTS, HALF), BF)] * 2 + [shape((SLOTS, FF), F32)] * 3,
        2_700_000_000,
        hbm_in=(2, 3, 4),
        grid_spec=spec,
        vmem=24 << 20,
    )(tp, own, gate_w, up_w, down_w)


def peer_body(
    tp, peer, gate_h, up_h, down_h, gate_o, up_o, act_o,
    rows_h, cot_h, active, pre_grad, up_grad, part,
    rows, cot, gate_w, up_w, down_w, sems, out_sems, acc,
):
    step, keep = open_step(
        1 - tp[0], peer, (gate_h, up_h, down_h), rows_h, cot_h, rows, cot, (gate_w, up_w, down_w),
        sems, out_sems,
    )
    for first in range(0, SLOTS, SLOTS // 2):
        at = slice(first, first + SLOTS // 2)
        gate_pre = gate_o[at] + mm(rows[at], gate_w[step], NN)
        up_val = up_o[at] + mm(rows[at], up_w[step], NN)
        act_grad = act_o[at] + mm(cot[at], down_w[step], NT)
        act, slope = silu_parts(gate_pre)
        active[at] = (act * up_val).astype(BF)
        up_grad[at] = (act_grad * act).astype(BF)
        pre_grad[at] = (act_grad * up_val * slope).astype(BF)
    for first in range(0, SLOTS, SLOTS // 2):
        at = slice(first, first + SLOTS // 2)
        before = jnp.where(step == 0, 0.0, acc[at])
        acc[at] = before + mm(pre_grad[at], gate_w[step], NT) + mm(up_grad[at], up_w[step], NT)

    @pl.when(step == 2)
    def _():
        part[...] = acc[...].astype(BF)
        for c in keep:
            c.wait()


def expert_peer(tp, peer, gate_w, up_w, down_w, gate_o, up_o, act_o):
    spec = pltpu.PrefetchScalarGridSpec(
        num_scalar_prefetch=1,
        grid=(FF // FF_STEP,),
        in_specs=[whole((MAIN, 2 * HALF + 256)), HBM, HBM, HBM]
        + [step_block((SLOTS, FF_STEP))] * 3,
        out_specs=[HBM, HBM] + [step_block((SLOTS, FF_STEP))] * 3 + [whole((SLOTS, HALF))],
        scratch_shapes=EXPERT_SCRATCH + [pltpu.VMEM((SLOTS, HALF), F32)],
    )
    return call(
        peer_body,
        [pltpu.HBM((SLOTS, HALF), BF)] * 2
        + [shape((SLOTS, FF))] * 3
        + [shape((SLOTS, HALF))],
        4_500_000_000,
        hbm_in=(2, 3, 4),
        grid_spec=spec,
        vmem=28 << 20,
    )(tp, peer, gate_w, up_w, down_w, gate_o, up_o, act_o)


def rows_body(tp, pre_grad, up_grad, gate_w, up_w, part):
    total = mm(pre_grad[...], gate_w[0], NT) + mm(up_grad[...], up_w[0], NT)
    part[...] = total.astype(BF)


def own_rows(tp, pre_grad, up_grad, gate_w, up_w):
    spec = pltpu.PrefetchScalarGridSpec(
        num_scalar_prefetch=1,
        grid=(4,),
        in_specs=[
            whole((SLOTS, FF)),
            whole((SLOTS, FF)),
            pl.BlockSpec((1, HALF // 4, FF), lambda i, t: (0, 4 * t[0] + i, 0)),
            pl.BlockSpec((1, HALF // 4, FF), lambda i, t: (0, 4 * t[0] + i, 0)),
        ],
        out_specs=step_block((SLOTS, HALF // 4)),
    )
    return call(
        rows_body, shape((SLOTS, HALF)), 1_800_000_000, grid_spec=spec, vmem=12 << 20
    )(tp, pre_grad, up_grad, gate_w, up_w)


def weight_body(tp, rows_o, cot_o, rows_p, cot_p, active, pre_grad, up_grad, gate_g, up_g, down_g):
    for half, rows, cot in ((0, rows_o, cot_o), (1, rows_p, cot_p)):

        @pl.when(pl.program_id(0) // 2 == half)
        def _():
            gate_g[0] = mm(rows[...], pre_grad[...], TN).astype(BF)
            up_g[0] = mm(rows[...], up_grad[...], TN).astype(BF)
            down_g[0] = mm(active[...], cot[...], TN).astype(BF)


def weight_grads(tp, rows_o, cot_o, rows_p, cot_p, active, pre_grad, up_grad):
    quarter = HALF // 2

    def block(i, t):
        return (t[0] * (1 - i // 2) + (1 - t[0]) * (i // 2)) * 2 + i % 2

    spec = pltpu.PrefetchScalarGridSpec(
        num_scalar_prefetch=1,
        grid=(4,),
        in_specs=[pl.BlockSpec((SLOTS, quarter), lambda i, t: (0, i % 2))] * 4
        + [whole((SLOTS, FF))] * 3,
        out_specs=[
            pl.BlockSpec((1, quarter, FF), lambda i, t: (0, block(i, t), 0)),
            pl.BlockSpec((1, quarter, FF), lambda i, t: (0, block(i, t), 0)),
            pl.BlockSpec((1, FF, quarter), lambda i, t: (0, 0, block(i, t))),
        ],
    )
    return call(
        weight_body,
        (shape((1, WIDTH, FF)), shape((1, WIDTH, FF)), shape((1, FF, WIDTH))),
        5_400_000_000,
        hbm_in=(1, 2, 3, 4),
        grid_spec=spec,
        vmem=24 << 20,
    )(tp, rows_o, cot_o, rows_p, cot_p, active, pre_grad, up_grad)


def reply_body(own, peer, states, out):
    total = (own[...].astype(F32) + peer[...].astype(F32)).astype(BF)
    out[:, 0:HALF] = total[:MAIN]
    out[:, HALF : HALF + 128] = fold_last(total[MAIN:])
    out[:, HALF + 128 :] = states[...]


def reply(own, peer, states):
    return call(reply_body, shape((MAIN, HALF + 128 + 384)), 100_000_000)(own, peer, states)


def scan_states(left_in, right_in, decays, out, work):
    def factor(b):
        at = 8 * b
        return decays[at : at + 1] + decays[at + 1 : at + 2] + decays[at + 2 : at + 3]

    factors = [factor(b) for b in range(BLOCKS)]
    left = jnp.zeros((8, 128), F32)
    right = jnp.zeros((8, 128), F32)
    for b in range(BLOCKS):
        at = 8 * b
        work[at : at + 8, 0:128] = left
        left = factors[b] * left + left_in[at : at + 8]
        back = BLOCKS - 1 - b
        at = 8 * back
        work[at : at + 8, 128:256] = right
        right = factors[back] * right + right_in[at : at + 8]
    out[:, 0:256] = work[...].astype(BF)


def join_body(tp, got, ids, cot, out, states, decays, work, wide):
    first, second = slot_choices(ids[...])
    both = ones_where(first | second)
    (last,) = unfold_last(got[:, HALF : HALF + 128])
    total = mm(both[:MAIN], got[:, :HALF], TN) + mm(both[MAIN:], last, TN)
    out[...] = (cot[...].astype(F32) + total).astype(BF)
    wide[...] = got[:, HALF + 128 :].astype(F32)
    decays[...] = wide[:, 256:]
    scan_states(wide[:, 0:128], wide[:, 128:256], wide[:, 256:], states, work)


def join(tp, got, ids, cot):
    spec = pltpu.PrefetchScalarGridSpec(
        num_scalar_prefetch=1,
        grid=(1,),
        in_specs=[
            whole((MAIN, HALF + 512)),
            whole((2, TOK)),
            pl.BlockSpec((TOK, HALF), lambda i, t: (0, t[0])),
        ],
        out_specs=[whole((TOK, HALF)), whole((MAIN, 256)), whole((MAIN, 128))],
        scratch_shapes=[pltpu.VMEM((MAIN, 256), F32), pltpu.VMEM((MAIN, 384), F32)],
    )
    return call(
        join_body,
        (shape((TOK, HALF)), shape((MAIN, 256)), shape((MAIN, 128), F32)),
        300_000_000,
        grid_spec=spec,
    )(tp, got, ids, cot)


def mix_body(
    stream, proj_w, gate_in, scan_out, start_w, end_w, out_map, x_states,
    gate_grad, scan_grad, gated, payload,
):
    mixed = mm(stream[0], proj_w[:, :HALF], NT) + mm(stream[1], proj_w[:, HALF:], NT)
    scan = scan_out[...].astype(F32)
    act, slope = silu_parts(gate_in[...].astype(F32))
    gated[...] = (scan * act).astype(BF)
    gate_grad[...] = (mixed * scan * slope).astype(BF)
    grad = (mixed * act).astype(BF)
    scan_grad[...] = grad
    wide = grad.astype(F32)
    block_states(
        payload, (end_w[...] * wide).astype(BF), (start_w[...] * wide).astype(BF), out_map
    )
    payload[:, 256:] = x_states[...]


def mix(*args):
    return call(
        mix_body,
        (shape((TOK, CHAN)), shape((TOK, CHAN)), shape((TOK, CHAN)), shape((MAIN, 512))),
        500_000_000,
    )(*args)


PARTS = ((0, 640), (1280, 384))


def proj_body(odd, stream, gated, keep, *sends):
    for i in range(2):
        part = mm(stream[i], gated[...], TN).reshape(32, 4, 8, CHAN)
        flat = [part[:, q].reshape(256, CHAN) for q in range(4)]
        rows = slice(256 * i, 256 * i + 256)

        def tile(t):
            return flat[t // 4][:, 128 * (t % 4) : 128 * (t % 4) + 128]

        at = 0
        for j, (first, width) in enumerate(PARTS):
            for k in range(width // 128):
                low = tile(first // 128 + k)
                high = tile((first + width) // 128 + k)
                upper = odd[j] == 1
                keep[rows, at : at + 128] = jnp.where(upper, high, low).astype(BF)
                sends[j][rows, 128 * k : 128 * k + 128] = jnp.where(upper, low, high).astype(BF)
                at += 128


def proj_part(odd, stream, gated):
    out = [pltpu.HBM((MAIN, 1024), BF)] + [shape((MAIN, width)) for _, width in PARTS]
    spec = pltpu.PrefetchScalarGridSpec(
        num_scalar_prefetch=1,
        grid=(1,),
        in_specs=[whole((2, TOK, HALF)), whole((TOK, CHAN))],
        out_specs=[whole(o.shape) for o in out],
    )
    return call(proj_body, out, 400_000_000, grid_spec=spec)(odd, stream, gated)


def scan_body(got, decays, keep_h, first, second, out, work, wide, keep, sem):
    fetch_keep = pltpu.make_async_copy(keep_h, keep, sem.at[0])
    fetch_keep.start()
    wide[...] = got[:, 0:256].astype(F32)
    scan_states(wide[:, 0:128], wide[:, 128:256], decays[...], out, work)
    fetch_keep.wait()
    at = 0
    for other in (first, second):
        width = other.shape[1]
        total = keep[:, at : at + width].astype(F32) + other[...].astype(F32)
        out[:, 256 + at : 256 + at + width] = total.astype(BF)
        at += width


def scan_grads(got, decays, keep, others):
    spec = pl.GridSpec(
        grid=(1,),
        in_specs=[whole((MAIN, 512)), whole((MAIN, 128)), HBM] + [whole(o.shape) for o in others],
        out_specs=whole((MAIN, 256 + 1024)),
        scratch_shapes=[
            pltpu.VMEM((MAIN, 256), F32),
            pltpu.VMEM((MAIN, 256), F32),
            pltpu.VMEM((MAIN, 1024), BF),
            pltpu.SemaphoreType.DMA((1,)),
        ],
    )
    return call(
        scan_body, shape((MAIN, 256 + 1024)), 100_000_000, hbm_in=(2,), grid_spec=spec
    )(got, decays, keep, *others)


def near_body(
    scan_grad, values, in_map, out_map, cum, cum_t, start_w, end_w, states,
    out_grad, value_part, in_part,
):
    wide = scan_grad[...].astype(F32)
    from_start = (start_w[...] * wide).astype(BF)
    to_end = (end_w[...] * wide).astype(BF)
    for g in range(2):
        keys = slice(128 * g, 128 * g + 128)
        chan = slice(256 * g, 256 * g + 256)
        in_keys = in_map[:, keys]
        out_keys = out_map[:, keys]
        meet = mm(out_keys, in_keys, NT)
        pair_sum = jnp.zeros((TOK, TOK), F32)
        for e in range(4):
            h = 4 * g + e
            at = slice(64 * h, 64 * h + 64)
            kernel = jnp.exp(-jnp.abs(cum[:, h : h + 1] - cum_t[h : h + 1, :]))
            grad = scan_grad[:, at]
            value_part[:, at] = mm((kernel * meet).astype(BF), grad, TN)
            pair_sum = pair_sum + kernel * mm(grad, values[:, at], NT)
        pair_sum = pair_sum.astype(BF)
        out_total = mm(pair_sum, in_keys, NN)
        out_total = out_total + mm(from_start[:, chan], states[chan, 0:128], NN)
        out_total = out_total + mm(to_end[:, chan], states[chan, 128:256], NN)
        out_grad[:, keys] = out_total.astype(BF)
        in_part[:, keys] = mm(pair_sum, out_keys, TN)


def near(*args):
    return call(
        near_body,
        (shape((TOK, KEYS)), shape((TOK, CHAN), F32), shape((TOK, KEYS), F32)),
        600_000_000,
    )(*args)


def far_body(
    tp, states, values_h, in_map_h, start_h, end_h, value_part_h, in_part_h,
    value_grad, in_grad, proj_grad,
    values, in_map, start_w, end_w, value_part, in_part, sems,
):
    pairs = (
        (values_h, values),
        (in_map_h, in_map),
        (start_h, start_w),
        (end_h, end_w),
        (value_part_h, value_part),
        (in_part_h, in_part),
    )
    copies = [pltpu.make_async_copy(a, b, sems.at[i]) for i, (a, b) in enumerate(pairs)]
    for c in copies:
        c.start()
    at = 256
    for j, (first, width) in enumerate(PARTS):
        sums = [[jnp.zeros((8, width), F32) for _ in range(2)] for _ in range(2)]
        for b in range(BLOCKS):
            chunk = states[8 * b : 8 * b + 8, at : at + width].astype(F32)
            here = sums[(b >> 4) & 1] if j == 0 else sums[b & 1]
            other = (b >> 2) & 1
            here[other] = here[other] + chunk
        at += width
        for half in range(2):
            total = sums[half][0] + sums[half][1]
            if j == 0:
                total = jnp.where(tp[0] == 0, total, sums[0][half] + sums[1][half])
            for k in range(width // 128):
                tile = (first + half * width) // 128 + k
                q, lane = 8 * (tile // 4), 128 * (tile % 4)
                proj_grad[q : q + 8, lane : lane + 128] = total[:, 128 * k : 128 * k + 128]
    for c in copies:
        c.wait()
    val = values[...].astype(F32)
    from_start = (start_w[...] * val).astype(BF)
    to_end = (end_w[...] * val).astype(BF)
    for g in range(2):
        keys = slice(128 * g, 128 * g + 128)
        chan = slice(256 * g, 256 * g + 256)
        in_keys = in_map[:, keys]
        left = states[chan, 0:128]
        right = states[chan, 128:256]
        total = value_part[:, chan] + start_w[:, chan] * mm(in_keys, left, NT)
        total = total + end_w[:, chan] * mm(in_keys, right, NT)
        value_grad[:, chan] = total.astype(BF)
        total = in_part[:, keys] + mm(from_start[:, chan], left, NN)
        total = total + mm(to_end[:, chan], right, NN)
        in_grad[:, keys] = total.astype(BF)


def far(*args):
    far_out = (shape((TOK, CHAN)), shape((TOK, KEYS)), shape((32, CHAN), F32))
    spec = pltpu.PrefetchScalarGridSpec(
        num_scalar_prefetch=1,
        grid=(1,),
        in_specs=[whole((MAIN, 256 + 1024))] + [pl.BlockSpec(memory_space=pltpu.HBM)] * 6,
        out_specs=[whole(o.shape) for o in far_out],
        scratch_shapes=[
            pltpu.VMEM((TOK, CHAN), BF),
            pltpu.VMEM((TOK, KEYS), BF),
            pltpu.VMEM((TOK, CHAN), F32),
            pltpu.VMEM((TOK, CHAN), F32),
            pltpu.VMEM((TOK, CHAN), F32),
            pltpu.VMEM((TOK, KEYS), F32),
            pltpu.SemaphoreType.DMA((6,)),
        ],
    )
    return call(far_body, far_out, 200_000_000, hbm_in=range(2, 8), grid_spec=spec)(*args)


def swap(rows):
    lanes = rows.shape[1]
    out = lax.all_to_all(rows.reshape(BLOCKS, -1, lanes), SP, 0, 0, tiled=True)
    return out.reshape(-1, lanes)


def pairs_of(piece):
    out = []
    for source in range(128):
        step = 2 if piece else 32 if source % 2 == 0 else 8
        out.append((source, source ^ step))
    return out


def other_core(array):
    return lax.ppermute(array, "tp", [(0, 1), (1, 0)])


def on_device(
    stream_rows,
    out_cotangent,
    expert_ids,
    route_weights,
    gate_weight,
    up_weight,
    down_weight,
    proj_weight,
    gate_input,
    scan_out,
    values,
    in_map,
    out_map,
    log_decay,
):
    tp = lax.axis_index("tp").astype(jnp.int32).reshape(1)
    ids = expert_ids.T
    sent = pack(tp, ids, route_weights.T, stream_rows, out_cotangent)
    own = swap(sent)
    x_payload, start_w, end_w, cum, cum_t = decay(values, in_map, log_decay.T)
    peer = other_core(own)
    rows_o, cot_o, *pre = expert_own(tp, own, gate_weight, up_weight, down_weight)
    rows_p, cot_p, active, pre_grad, up_grad, part_peer = expert_peer(
        tp, peer, gate_weight, up_weight, down_weight, *pre
    )
    part_in = other_core(part_peer)
    part_own = own_rows(tp, pre_grad, up_grad, gate_weight, up_weight)
    sent_back = reply(part_own, part_in, x_payload)
    back = swap(sent_back)
    gate_w_grad, up_w_grad, down_grad = weight_grads(
        tp, rows_o, cot_o, rows_p, cot_p, active, pre_grad, up_grad
    )
    stream_grad, x_states, decays = join(tp, back, ids, out_cotangent)
    stream = lax.all_gather(stream_grad, "tp")
    gate_grad, scan_grad, gated, payload = mix(
        stream, proj_weight, gate_input, scan_out, start_w, end_w, out_map, x_states
    )
    got = swap(payload)
    place = [lax.axis_index(name).astype(jnp.int32) & 1 for name in SP]
    odd = jnp.stack([jnp.where(tp[0] == 0, place[0], place[1]), place[2]])
    keep, *halves = proj_part(odd, stream, gated)
    others = [lax.ppermute(h, ALL, pairs_of(i)) for i, h in enumerate(halves)]
    buffer = scan_grads(got, decays, keep, others)
    g_states = swap(buffer)
    out_grad, value_part, in_part = near(
        scan_grad, values, in_map, out_map, cum, cum_t, start_w, end_w, got[:, 256:]
    )
    value_grad, in_grad, proj_grad = far(
        tp, g_states, values, in_map, start_w, end_w, value_part, in_part
    )
    return (
        stream_grad,
        proj_grad,
        value_grad,
        in_grad,
        out_grad,
        gate_grad,
        gate_w_grad,
        up_w_grad,
        down_grad,
    )


def solution(mesh):
    finer = Mesh(mesh.devices.reshape(4, 4, 4, mesh.shape["tp"]), ("sp_0", "sp_1", "sp_2", "tp"))
    return jax.shard_map(
        on_device,
        mesh=finer,
        in_specs=(
            P(SP, None),
            P(SP, None),
            P(SP, None),
            P(SP, None),
            P(SP, None, "tp"),
            P(SP, None, "tp"),
            P(SP, "tp", None),
            P("tp", None),
            P(SP, "tp"),
            P(SP, "tp"),
            P(SP, "tp"),
            P(SP, "tp"),
            P(SP, "tp"),
            P(SP, "tp"),
        ),
        out_specs=(
            P(SP, "tp"),
            P(SP, "tp"),
            P(SP, "tp"),
            P(SP, "tp"),
            P(SP, "tp"),
            P(SP, "tp"),
            P(SP, None, "tp"),
            P(SP, None, "tp"),
            P(SP, "tp", None),
        ),
        check_vma=False,
    )
```

```python
import jax
import jax.numpy as jnp
from jax import lax
from jax.experimental import pallas as pl
from jax.experimental.pallas import tpu as pltpu
from jax.sharding import Mesh
from jax.sharding import PartitionSpec as P


SP = ("sp_0", "sp_1", "sp_2")
ALL = SP + ("tp",)
TOK = 192
WIDTH = 2048
HALF = 1024
EXPERTS = 64
MAIN = 512
SLOTS = 576
FF = 768
FF_STEP = 256
CHAN = 512
KEYS = 256
HEADS = 8
BLOCKS = 64

BF = jnp.bfloat16
F32 = jnp.float32
EXACT = lax.Precision.HIGHEST


def mm(a, b, dims, precision=None):
    return lax.dot_general(a, b, (dims, ((), ())), preferred_element_type=F32, precision=precision)


NN = ((1,), (0,))
NT = ((1,), (1,))
TN = ((0,), (0,))


def iota(shape, dim):
    return lax.broadcasted_iota(jnp.int32, shape, dim)


def ones_where(mask):
    return jnp.where(mask, 1.0, 0.0).astype(BF)


def call(body, out_shape, flops, hbm_in=(), **kw):
    vmem = kw.pop("vmem", 12 << 20)
    kernel = pl.pallas_call(
        body,
        out_shape=out_shape,
        compiler_params=pltpu.CompilerParams(vmem_limit_bytes=vmem),
        cost_estimate=pl.CostEstimate(flops=flops, bytes_accessed=1 << 20, transcendentals=0),
        **kw,
    )

    def run(*args):
        return kernel(
            *[
                pltpu.with_memory_space_constraint(a, pltpu.HBM) if i in hbm_in else a
                for i, a in enumerate(args)
            ]
        )

    return run


def shape(dims, dtype=BF):
    return jax.ShapeDtypeStruct(dims, dtype)


def slot_choices(ids):
    expert = iota((EXPERTS, TOK), 0)
    named = [ids[k : k + 1] == expert for k in range(2)]
    either = ones_where(named[0] | named[1])
    earlier = ones_where(iota((TOK, TOK), 0) < iota((TOK, TOK), 1))
    count = mm(either, earlier, NN)
    picks = []
    for k in range(2):
        rank = jnp.sum(jnp.where(named[k], count, 0.0), axis=0, keepdims=True).astype(jnp.int32)
        own = ids[k : k + 1]
        row = jnp.where(rank < 8, own * 8 + rank, MAIN + own)
        picks.append(row == iota((SLOTS, TOK), 0))
    return picks


def fold_last(rows):
    q = iota((MAIN, MAIN), 0)
    order = ones_where(iota((MAIN, MAIN), 1) == (q & 7) * EXPERTS + (q >> 3))
    stacked = jnp.concatenate([rows[:, 128 * j : 128 * j + 128] for j in range(8)], axis=0)
    return mm(order, stacked, NN).astype(BF)


def unfold_last(folded):
    c = iota((MAIN, MAIN), 0)
    order = ones_where(iota((MAIN, MAIN), 1) == (c & 63) * 8 + (c >> 6))
    stacked = mm(order, folded, NN).astype(BF)
    return [
        jnp.concatenate(
            [stacked[64 * j : 64 * j + 64, 128 * i : 128 * i + 128] for j in range(8)], axis=1
        )
        for i in range(folded.shape[1] // 128)
    ]


def pack_body(tp, ids, weights, rows_hbm, cot_hbm, out_hbm, rows, cot, out, sems):
    at = pl.ds(pl.multiple_of(tp[0] * HALF, HALF), HALF)
    get_rows = pltpu.make_async_copy(rows_hbm.at[:, at], rows, sems.at[0])
    get_cot = pltpu.make_async_copy(cot_hbm.at[:, at], cot, sems.at[1])
    get_rows.start()
    get_cot.start()
    first, second = slot_choices(ids[...])
    both = ones_where(first | second)
    scale = jnp.where(first, weights[0:1], jnp.where(second, weights[1:2], 0.0))
    scale = jnp.sum(scale, axis=1, keepdims=True)

    def leave(k, low, high):
        lanes = slice(low, high)
        return pltpu.make_async_copy(out.at[:, lanes], out_hbm.at[:, lanes], sems.at[k])

    pieces = (leave(2, 0, HALF), leave(3, HALF, 2 * HALF), leave(4, 2 * HALF, 2 * HALF + 256))
    get_rows.wait()
    row_slots = mm(both, rows[...], NN).astype(BF)
    out[:, 0:HALF] = row_slots[:MAIN]
    pieces[0].start()
    out[:, 2 * HALF : 2 * HALF + 128] = fold_last(row_slots[MAIN:])
    get_cot.wait()
    cot_slots = (scale * mm(both, cot[...], NN)).astype(BF)
    out[:, 2 * HALF + 128 :] = fold_last(cot_slots[MAIN:])
    pieces[2].start()
    out[:, HALF : 2 * HALF] = cot_slots[:MAIN]
    pieces[1].start()
    for piece in pieces:
        piece.wait()


def whole(dims):
    return pl.BlockSpec(dims, lambda *_: (0,) * len(dims))


def pack(tp, ids, weights, rows, cot):
    spec = pltpu.PrefetchScalarGridSpec(
        num_scalar_prefetch=1,
        grid=(1,),
        in_specs=[
            whole((2, TOK)),
            whole((2, TOK)),
            pl.BlockSpec(memory_space=pltpu.HBM),
            pl.BlockSpec(memory_space=pltpu.HBM),
        ],
        out_specs=pl.BlockSpec(memory_space=pltpu.HBM),
        scratch_shapes=[
            pltpu.VMEM((TOK, HALF), BF),
            pltpu.VMEM((TOK, HALF), BF),
            pltpu.VMEM((MAIN, 2 * HALF + 256), BF),
            pltpu.SemaphoreType.DMA((5,)),
        ],
    )
    return call(
        pack_body, pltpu.HBM((MAIN, 2 * HALF + 256), BF), 1_000_000_000, hbm_in=(1, 2, 3, 4), grid_spec=spec
    )(tp, ids, weights, rows, cot)


def decay_body(values, in_map, log_decay, payload, start_w, end_w, cum_out, cum_t_out):
    upto = jnp.where(iota((TOK, TOK), 0) <= iota((TOK, TOK), 1), 1.0, 0.0)
    cum = mm(upto, log_decay[...], ((0,), (1,)), EXACT)
    cum_t = mm(log_decay[...], upto, NN, EXACT)
    cum_out[...] = cum
    cum_t_out[...] = cum_t
    spread = jnp.where(iota((HEADS, CHAN), 1) // 64 == iota((HEADS, CHAN), 0), 1.0, 0.0)
    from_start = mm(jnp.exp(cum), spread, NN, EXACT)
    to_end = mm(jnp.exp(cum[TOK - 1 :, :] - cum), spread, NN, EXACT)
    start_w[...] = from_start
    end_w[...] = to_end
    val = values[...].astype(F32)
    block_states(payload, (to_end * val).astype(BF), (from_start * val).astype(BF), in_map)
    total = jnp.exp(cum_t[:, TOK - 1 :])
    total = jnp.concatenate(
        [jnp.broadcast_to(total[h : h + 1], (64, 128)) for h in range(HEADS)], axis=0
    )
    high = total.astype(BF)
    rest = total - high.astype(F32)
    mid = rest.astype(BF)
    low = (rest - mid.astype(F32)).astype(BF)
    part = iota((MAIN, 128), 0) & 7
    parts = jnp.where(part == 0, high.astype(F32), 0.0)
    parts = jnp.where(part == 1, mid.astype(F32), parts)
    parts = jnp.where(part == 2, low.astype(F32), parts)
    payload[:, 256:] = parts.astype(BF)


def block_states(payload, to_end, from_start, keys):
    for g in range(2):
        chan = slice(256 * g, 256 * g + 256)
        key = keys[:, 128 * g : 128 * g + 128]
        payload[chan, 0:128] = mm(to_end[:, chan], key, TN).astype(BF)
        payload[chan, 128:256] = mm(from_start[:, chan], key, TN).astype(BF)


def decay(values, in_map, log_decay):
    return call(
        decay_body,
        (
            shape((MAIN, 384)),
            shape((TOK, CHAN), F32),
            shape((TOK, CHAN), F32),
            shape((TOK, HEADS), F32),
            shape((HEADS, TOK), F32),
        ),
        1_000_000_000,
    )(values, in_map, log_decay)


def silu_parts(x):
    squash = 0.5 * jnp.tanh(0.5 * x) + 0.5
    return x * squash, squash * (1.0 + x * (1.0 - squash))


def split_slots(got, rows, cot):
    rows[:MAIN] = got[:, 0:HALF]
    cot[:MAIN] = got[:, HALF : 2 * HALF]
    last_rows, last_cot = unfold_last(got[:, 2 * HALF :])
    rows[MAIN:] = last_rows
    cot[MAIN:] = last_cot


def fetch(half, gate_h, up_h, down_h, gate_w, up_w, down_w, sems):
    wide = pl.ds(pl.multiple_of(half * HALF, HALF), HALF)
    steps = []
    for j in range(FF // FF_STEP):
        part = pl.ds(j * FF_STEP, FF_STEP)
        steps.append(
            (
                pltpu.make_async_copy(gate_h.at[0, wide, part], gate_w.at[j], sems.at[j, 0]),
                pltpu.make_async_copy(up_h.at[0, wide, part], up_w.at[j], sems.at[j, 1]),
                pltpu.make_async_copy(down_h.at[0, part, wide], down_w.at[j], sems.at[j, 2]),
            )
        )
    return steps


def open_step(half, got, weights_h, rows_h, cot_h, rows, cot, weights, sems, out_sems):
    step = pl.program_id(0)
    copies = fetch(half, *weights_h, *weights, sems)
    keep = (
        pltpu.make_async_copy(rows, rows_h, out_sems.at[0]),
        pltpu.make_async_copy(cot, cot_h, out_sems.at[1]),
    )

    def start(group):
        for c in group:
            c.start()

    @pl.when(step == 0)
    def _():
        start(copies[0])
        split_slots(got, rows, cot)

    for j, group in enumerate(copies):

        @pl.when(step == j)
        def _():
            for c in group:
                c.wait()
            if j == 0:
                start(copies[1])
            if j == 1:
                start(keep)
            if j < 1:
                start(copies[2])

    return step, keep


def own_body(
    tp, own, gate_h, up_h, down_h, rows_h, cot_h, gate_o, up_o, act_o,
    rows, cot, gate_w, up_w, down_w, sems, out_sems,
):
    step, keep = open_step(
        tp[0], own, (gate_h, up_h, down_h), rows_h, cot_h, rows, cot, (gate_w, up_w, down_w),
        sems, out_sems,
    )
    for first in range(0, SLOTS, SLOTS // 2):
        at = slice(first, first + SLOTS // 2)
        gate_o[at] = mm(rows[at], gate_w[step], NN)
        up_o[at] = mm(rows[at], up_w[step], NN)
        act_o[at] = mm(cot[at], down_w[step], NT)

    @pl.when(step == 2)
    def _():
        for c in keep:
            c.wait()


def step_block(dims):
    return pl.BlockSpec(dims, lambda i, t: (0, i))


HBM = pl.BlockSpec(memory_space=pltpu.HBM)
EXPERT_SCRATCH = [
    pltpu.VMEM((SLOTS, HALF), BF),
    pltpu.VMEM((SLOTS, HALF), BF),
    pltpu.VMEM((3, HALF, FF_STEP), BF),
    pltpu.VMEM((3, HALF, FF_STEP), BF),
    pltpu.VMEM((3, FF_STEP, HALF), BF),
    pltpu.SemaphoreType.DMA((3, 3)),
    pltpu.SemaphoreType.DMA((2,)),
]


def expert_own(tp, own, gate_w, up_w, down_w):
    spec = pltpu.PrefetchScalarGridSpec(
        num_scalar_prefetch=1,
        grid=(FF // FF_STEP,),
        in_specs=[whole((MAIN, 2 * HALF + 256)), HBM, HBM, HBM],
        out_specs=[HBM, HBM] + [step_block((SLOTS, FF_STEP))] * 3,
        scratch_shapes=EXPERT_SCRATCH,
    )
    return call(
        own_body,
        [pltpu.HBM((SLOTS, HALF), BF)] * 2 + [shape((SLOTS, FF), F32)] * 3,
        2_700_000_000,
        hbm_in=(2, 3, 4),
        grid_spec=spec,
        vmem=24 << 20,
    )(tp, own, gate_w, up_w, down_w)


def peer_body(
    tp, peer, gate_h, up_h, down_h, gate_o, up_o, act_o,
    rows_h, cot_h, active, pre_grad, up_grad, part,
    rows, cot, gate_w, up_w, down_w, sems, out_sems, acc,
):
    step, keep = open_step(
        1 - tp[0], peer, (gate_h, up_h, down_h), rows_h, cot_h, rows, cot, (gate_w, up_w, down_w),
        sems, out_sems,
    )
    for first in range(0, SLOTS, SLOTS // 2):
        at = slice(first, first + SLOTS // 2)
        gate_pre = gate_o[at] + mm(rows[at], gate_w[step], NN)
        up_val = up_o[at] + mm(rows[at], up_w[step], NN)
        act_grad = act_o[at] + mm(cot[at], down_w[step], NT)
        act, slope = silu_parts(gate_pre)
        active[at] = (act * up_val).astype(BF)
        up_grad[at] = (act_grad * act).astype(BF)
        pre_grad[at] = (act_grad * up_val * slope).astype(BF)
    for first in range(0, SLOTS, SLOTS // 2):
        at = slice(first, first + SLOTS // 2)
        before = jnp.where(step == 0, 0.0, acc[at])
        acc[at] = before + mm(pre_grad[at], gate_w[step], NT) + mm(up_grad[at], up_w[step], NT)

    @pl.when(step == 2)
    def _():
        part[...] = acc[...].astype(BF)
        for c in keep:
            c.wait()


def expert_peer(tp, peer, gate_w, up_w, down_w, gate_o, up_o, act_o):
    spec = pltpu.PrefetchScalarGridSpec(
        num_scalar_prefetch=1,
        grid=(FF // FF_STEP,),
        in_specs=[whole((MAIN, 2 * HALF + 256)), HBM, HBM, HBM]
        + [step_block((SLOTS, FF_STEP))] * 3,
        out_specs=[HBM, HBM] + [step_block((SLOTS, FF_STEP))] * 3 + [whole((SLOTS, HALF))],
        scratch_shapes=EXPERT_SCRATCH + [pltpu.VMEM((SLOTS, HALF), F32)],
    )
    return call(
        peer_body,
        [pltpu.HBM((SLOTS, HALF), BF)] * 2
        + [shape((SLOTS, FF))] * 3
        + [shape((SLOTS, HALF))],
        4_500_000_000,
        hbm_in=(2, 3, 4),
        grid_spec=spec,
        vmem=28 << 20,
    )(tp, peer, gate_w, up_w, down_w, gate_o, up_o, act_o)


def rows_body(tp, pre_grad, up_grad, gate_w, up_w, part):
    total = mm(pre_grad[...], gate_w[0], NT) + mm(up_grad[...], up_w[0], NT)
    part[...] = total.astype(BF)


def own_rows(tp, pre_grad, up_grad, gate_w, up_w):
    spec = pltpu.PrefetchScalarGridSpec(
        num_scalar_prefetch=1,
        grid=(4,),
        in_specs=[
            whole((SLOTS, FF)),
            whole((SLOTS, FF)),
            pl.BlockSpec((1, HALF // 4, FF), lambda i, t: (0, 4 * t[0] + i, 0)),
            pl.BlockSpec((1, HALF // 4, FF), lambda i, t: (0, 4 * t[0] + i, 0)),
        ],
        out_specs=step_block((SLOTS, HALF // 4)),
    )
    return call(
        rows_body, shape((SLOTS, HALF)), 1_800_000_000, grid_spec=spec, vmem=12 << 20
    )(tp, pre_grad, up_grad, gate_w, up_w)


def weight_body(tp, rows_o, cot_o, rows_p, cot_p, active, pre_grad, up_grad, gate_g, up_g, down_g):
    for half, rows, cot in ((0, rows_o, cot_o), (1, rows_p, cot_p)):

        @pl.when(pl.program_id(0) // 2 == half)
        def _():
            gate_g[0] = mm(rows[...], pre_grad[...], TN).astype(BF)
            up_g[0] = mm(rows[...], up_grad[...], TN).astype(BF)
            down_g[0] = mm(active[...], cot[...], TN).astype(BF)


def weight_grads(tp, rows_o, cot_o, rows_p, cot_p, active, pre_grad, up_grad):
    quarter = HALF // 2

    def block(i, t):
        return (t[0] * (1 - i // 2) + (1 - t[0]) * (i // 2)) * 2 + i % 2

    spec = pltpu.PrefetchScalarGridSpec(
        num_scalar_prefetch=1,
        grid=(4,),
        in_specs=[pl.BlockSpec((SLOTS, quarter), lambda i, t: (0, i % 2))] * 4
        + [whole((SLOTS, FF))] * 3,
        out_specs=[
            pl.BlockSpec((1, quarter, FF), lambda i, t: (0, block(i, t), 0)),
            pl.BlockSpec((1, quarter, FF), lambda i, t: (0, block(i, t), 0)),
            pl.BlockSpec((1, FF, quarter), lambda i, t: (0, 0, block(i, t))),
        ],
    )
    return call(
        weight_body,
        (shape((1, WIDTH, FF)), shape((1, WIDTH, FF)), shape((1, FF, WIDTH))),
        5_400_000_000,
        hbm_in=(1, 2, 3, 4),
        grid_spec=spec,
        vmem=24 << 20,
    )(tp, rows_o, cot_o, rows_p, cot_p, active, pre_grad, up_grad)


def reply_body(own, peer, states, out):
    total = (own[...].astype(F32) + peer[...].astype(F32)).astype(BF)
    out[:, 0:HALF] = total[:MAIN]
    out[:, HALF : HALF + 128] = fold_last(total[MAIN:])
    out[:, HALF + 128 :] = states[...]


def reply(own, peer, states):
    return call(reply_body, shape((MAIN, HALF + 128 + 384)), 100_000_000)(own, peer, states)


def scan_states(left_in, right_in, decays, out, work):
    def factor(b):
        at = 8 * b
        return decays[at : at + 1] + decays[at + 1 : at + 2] + decays[at + 2 : at + 3]

    factors = [factor(b) for b in range(BLOCKS)]
    left = jnp.zeros((8, 128), F32)
    right = jnp.zeros((8, 128), F32)
    for b in range(BLOCKS):
        at = 8 * b
        work[at : at + 8, 0:128] = left
        left = factors[b] * left + left_in[at : at + 8]
        back = BLOCKS - 1 - b
        at = 8 * back
        work[at : at + 8, 128:256] = right
        right = factors[back] * right + right_in[at : at + 8]
    out[:, 0:256] = work[...].astype(BF)


def join_body(tp, got, ids, cot, out, states, decays, work, wide):
    first, second = slot_choices(ids[...])
    both = ones_where(first | second)
    (last,) = unfold_last(got[:, HALF : HALF + 128])
    total = mm(both[:MAIN], got[:, :HALF], TN) + mm(both[MAIN:], last, TN)
    out[...] = (cot[...].astype(F32) + total).astype(BF)
    wide[...] = got[:, HALF + 128 :].astype(F32)
    decays[...] = wide[:, 256:]
    scan_states(wide[:, 0:128], wide[:, 128:256], wide[:, 256:], states, work)


def join(tp, got, ids, cot):
    spec = pltpu.PrefetchScalarGridSpec(
        num_scalar_prefetch=1,
        grid=(1,),
        in_specs=[
            whole((MAIN, HALF + 512)),
            whole((2, TOK)),
            pl.BlockSpec((TOK, HALF), lambda i, t: (0, t[0])),
        ],
        out_specs=[whole((TOK, HALF)), whole((MAIN, 256)), whole((MAIN, 128))],
        scratch_shapes=[pltpu.VMEM((MAIN, 256), F32), pltpu.VMEM((MAIN, 384), F32)],
    )
    return call(
        join_body,
        (shape((TOK, HALF)), shape((MAIN, 256)), shape((MAIN, 128), F32)),
        300_000_000,
        grid_spec=spec,
    )(tp, got, ids, cot)


def mix_body(
    stream, proj_w, gate_in, scan_out, start_w, end_w, out_map, x_states,
    gate_grad, scan_grad, gated, payload,
):
    mixed = mm(stream[0], proj_w[:, :HALF], NT) + mm(stream[1], proj_w[:, HALF:], NT)
    scan = scan_out[...].astype(F32)
    act, slope = silu_parts(gate_in[...].astype(F32))
    gated[...] = (scan * act).astype(BF)
    gate_grad[...] = (mixed * scan * slope).astype(BF)
    grad = (mixed * act).astype(BF)
    scan_grad[...] = grad
    wide = grad.astype(F32)
    block_states(
        payload, (end_w[...] * wide).astype(BF), (start_w[...] * wide).astype(BF), out_map
    )
    payload[:, 256:] = x_states[...]


def mix(*args):
    return call(
        mix_body,
        (shape((TOK, CHAN)), shape((TOK, CHAN)), shape((TOK, CHAN)), shape((MAIN, 512))),
        500_000_000,
    )(*args)


PARTS = ((0, 640), (1280, 384))


def proj_body(odd, stream, gated, keep, *sends):
    for i in range(2):
        part = mm(stream[i], gated[...], TN).reshape(32, 4, 8, CHAN)
        flat = [part[:, q].reshape(256, CHAN) for q in range(4)]
        rows = slice(256 * i, 256 * i + 256)

        def tile(t):
            return flat[t // 4][:, 128 * (t % 4) : 128 * (t % 4) + 128]

        at = 0
        for j, (first, width) in enumerate(PARTS):
            for k in range(width // 128):
                low = tile(first // 128 + k)
                high = tile((first + width) // 128 + k)
                upper = odd[j] == 1
                keep[rows, at : at + 128] = jnp.where(upper, high, low).astype(BF)
                sends[j][rows, 128 * k : 128 * k + 128] = jnp.where(upper, low, high).astype(BF)
                at += 128


def proj_part(odd, stream, gated):
    out = [pltpu.HBM((MAIN, 1024), BF)] + [shape((MAIN, width)) for _, width in PARTS]
    spec = pltpu.PrefetchScalarGridSpec(
        num_scalar_prefetch=1,
        grid=(1,),
        in_specs=[whole((2, TOK, HALF)), whole((TOK, CHAN))],
        out_specs=[whole(o.shape) for o in out],
    )
    return call(proj_body, out, 400_000_000, grid_spec=spec)(odd, stream, gated)


def scan_body(got, decays, keep_h, first, second, out, work, wide, keep, sem):
    fetch_keep = pltpu.make_async_copy(keep_h, keep, sem.at[0])
    fetch_keep.start()
    wide[...] = got[:, 0:256].astype(F32)
    scan_states(wide[:, 0:128], wide[:, 128:256], decays[...], out, work)
    fetch_keep.wait()
    at = 0
    for other in (first, second):
        width = other.shape[1]
        total = keep[:, at : at + width].astype(F32) + other[...].astype(F32)
        out[:, 256 + at : 256 + at + width] = total.astype(BF)
        at += width


def scan_grads(got, decays, keep, others):
    spec = pl.GridSpec(
        grid=(1,),
        in_specs=[whole((MAIN, 512)), whole((MAIN, 128)), HBM] + [whole(o.shape) for o in others],
        out_specs=whole((MAIN, 256 + 1024)),
        scratch_shapes=[
            pltpu.VMEM((MAIN, 256), F32),
            pltpu.VMEM((MAIN, 256), F32),
            pltpu.VMEM((MAIN, 1024), BF),
            pltpu.SemaphoreType.DMA((1,)),
        ],
    )
    return call(
        scan_body, shape((MAIN, 256 + 1024)), 100_000_000, hbm_in=(2,), grid_spec=spec
    )(got, decays, keep, *others)


def near_body(
    scan_grad, values, in_map, out_map, cum, cum_t, start_w, end_w, states,
    out_grad, value_part, in_part,
):
    wide = scan_grad[...].astype(F32)
    from_start = (start_w[...] * wide).astype(BF)
    to_end = (end_w[...] * wide).astype(BF)
    for g in range(2):
        keys = slice(128 * g, 128 * g + 128)
        chan = slice(256 * g, 256 * g + 256)
        in_keys = in_map[:, keys]
        out_keys = out_map[:, keys]
        meet = mm(out_keys, in_keys, NT)
        pair_sum = jnp.zeros((TOK, TOK), F32)
        for e in range(4):
            h = 4 * g + e
            at = slice(64 * h, 64 * h + 64)
            kernel = jnp.exp(-jnp.abs(cum[:, h : h + 1] - cum_t[h : h + 1, :]))
            grad = scan_grad[:, at]
            value_part[:, at] = mm((kernel * meet).astype(BF), grad, TN)
            pair_sum = pair_sum + kernel * mm(grad, values[:, at], NT)
        pair_sum = pair_sum.astype(BF)
        out_total = mm(pair_sum, in_keys, NN)
        out_total = out_total + mm(from_start[:, chan], states[chan, 0:128], NN)
        out_total = out_total + mm(to_end[:, chan], states[chan, 128:256], NN)
        out_grad[:, keys] = out_total.astype(BF)
        in_part[:, keys] = mm(pair_sum, out_keys, TN)


def near(*args):
    return call(
        near_body,
        (shape((TOK, KEYS)), shape((TOK, CHAN), F32), shape((TOK, KEYS), F32)),
        600_000_000,
    )(*args)


def far_body(
    tp, states, values_h, in_map_h, start_h, end_h, value_part_h, in_part_h,
    value_grad, in_grad, proj_grad,
    values, in_map, start_w, end_w, value_part, in_part, sems,
):
    pairs = (
        (values_h, values),
        (in_map_h, in_map),
        (start_h, start_w),
        (end_h, end_w),
        (value_part_h, value_part),
        (in_part_h, in_part),
    )
    copies = [pltpu.make_async_copy(a, b, sems.at[i]) for i, (a, b) in enumerate(pairs)]
    for c in copies:
        c.start()
    at = 256
    for j, (first, width) in enumerate(PARTS):
        sums = [[jnp.zeros((8, width), F32) for _ in range(2)] for _ in range(2)]
        for b in range(BLOCKS):
            chunk = states[8 * b : 8 * b + 8, at : at + width].astype(F32)
            here = sums[(b >> 4) & 1] if j == 0 else sums[b & 1]
            other = (b >> 2) & 1
            here[other] = here[other] + chunk
        at += width
        for half in range(2):
            total = sums[half][0] + sums[half][1]
            if j == 0:
                total = jnp.where(tp[0] == 0, total, sums[0][half] + sums[1][half])
            for k in range(width // 128):
                tile = (first + half * width) // 128 + k
                q, lane = 8 * (tile // 4), 128 * (tile % 4)
                proj_grad[q : q + 8, lane : lane + 128] = total[:, 128 * k : 128 * k + 128]
    for c in copies:
        c.wait()
    val = values[...].astype(F32)
    from_start = (start_w[...] * val).astype(BF)
    to_end = (end_w[...] * val).astype(BF)
    for g in range(2):
        keys = slice(128 * g, 128 * g + 128)
        chan = slice(256 * g, 256 * g + 256)
        in_keys = in_map[:, keys]
        left = states[chan, 0:128]
        right = states[chan, 128:256]
        total = value_part[:, chan] + start_w[:, chan] * mm(in_keys, left, NT)
        total = total + end_w[:, chan] * mm(in_keys, right, NT)
        value_grad[:, chan] = total.astype(BF)
        total = in_part[:, keys] + mm(from_start[:, chan], left, NN)
        total = total + mm(to_end[:, chan], right, NN)
        in_grad[:, keys] = total.astype(BF)


def far(*args):
    far_out = (shape((TOK, CHAN)), shape((TOK, KEYS)), shape((32, CHAN), F32))
    spec = pltpu.PrefetchScalarGridSpec(
        num_scalar_prefetch=1,
        grid=(1,),
        in_specs=[whole((MAIN, 256 + 1024))] + [pl.BlockSpec(memory_space=pltpu.HBM)] * 6,
        out_specs=[whole(o.shape) for o in far_out],
        scratch_shapes=[
            pltpu.VMEM((TOK, CHAN), BF),
            pltpu.VMEM((TOK, KEYS), BF),
            pltpu.VMEM((TOK, CHAN), F32),
            pltpu.VMEM((TOK, CHAN), F32),
            pltpu.VMEM((TOK, CHAN), F32),
            pltpu.VMEM((TOK, KEYS), F32),
            pltpu.SemaphoreType.DMA((6,)),
        ],
    )
    return call(far_body, far_out, 200_000_000, hbm_in=range(2, 8), grid_spec=spec)(*args)


def swap(rows):
    lanes = rows.shape[1]
    out = lax.all_to_all(rows.reshape(BLOCKS, -1, lanes), SP, 0, 0, tiled=True)
    return out.reshape(-1, lanes)


def pairs_of(piece):
    out = []
    for source in range(128):
        step = 2 if piece else 32 if source % 2 == 0 else 8
        out.append((source, source ^ step))
    return out


def other_core(array):
    return lax.ppermute(array, "tp", [(0, 1), (1, 0)])


def on_device(
    stream_rows,
    out_cotangent,
    expert_ids,
    route_weights,
    gate_weight,
    up_weight,
    down_weight,
    proj_weight,
    gate_input,
    scan_out,
    values,
    in_map,
    out_map,
    log_decay,
):
    tp = lax.axis_index("tp").astype(jnp.int32).reshape(1)
    ids = expert_ids.T
    sent = pack(tp, ids, route_weights.T, stream_rows, out_cotangent)
    own = swap(sent)
    x_payload, start_w, end_w, cum, cum_t = decay(values, in_map, log_decay.T)
    peer = other_core(own)
    rows_o, cot_o, *pre = expert_own(tp, own, gate_weight, up_weight, down_weight)
    rows_p, cot_p, active, pre_grad, up_grad, part_peer = expert_peer(
        tp, peer, gate_weight, up_weight, down_weight, *pre
    )
    part_in = other_core(part_peer)
    part_own = own_rows(tp, pre_grad, up_grad, gate_weight, up_weight)
    sent_back = reply(part_own, part_in, x_payload)
    back = swap(sent_back)
    gate_w_grad, up_w_grad, down_grad = weight_grads(
        tp, rows_o, cot_o, rows_p, cot_p, active, pre_grad, up_grad
    )
    stream_grad, x_states, decays = join(tp, back, ids, out_cotangent)
    stream = lax.all_gather(stream_grad, "tp")
    gate_grad, scan_grad, gated, payload = mix(
        stream, proj_weight, gate_input, scan_out, start_w, end_w, out_map, x_states
    )
    got = swap(payload)
    place = [lax.axis_index(name).astype(jnp.int32) & 1 for name in SP]
    odd = jnp.stack([jnp.where(tp[0] == 0, place[0], place[1]), place[2]])
    keep, *halves = proj_part(odd, stream, gated)
    others = [lax.ppermute(h, ALL, pairs_of(i)) for i, h in enumerate(halves)]
    buffer = scan_grads(got, decays, keep, others)
    g_states = swap(buffer)
    out_grad, value_part, in_part = near(
        scan_grad, values, in_map, out_map, cum, cum_t, start_w, end_w, got[:, 256:]
    )
    value_grad, in_grad, proj_grad = far(
        tp, g_states, values, in_map, start_w, end_w, value_part, in_part
    )
    return (
        stream_grad,
        proj_grad,
        value_grad,
        in_grad,
        out_grad,
        gate_grad,
        gate_w_grad,
        up_w_grad,
        down_grad,
    )


def solution(mesh):
    finer = Mesh(mesh.devices.reshape(4, 4, 4, mesh.shape["tp"]), ("sp_0", "sp_1", "sp_2", "tp"))
    return jax.shard_map(
        on_device,
        mesh=finer,
        in_specs=(
            P(SP, None),
            P(SP, None),
            P(SP, None),
            P(SP, None),
            P(SP, None, "tp"),
            P(SP, None, "tp"),
            P(SP, "tp", None),
            P("tp", None),
            P(SP, "tp"),
            P(SP, "tp"),
            P(SP, "tp"),
            P(SP, "tp"),
            P(SP, "tp"),
            P(SP, "tp"),
        ),
        out_specs=(
            P(SP, "tp"),
            P(SP, "tp"),
            P(SP, "tp"),
            P(SP, "tp"),
            P(SP, "tp"),
            P(SP, "tp"),
            P(SP, None, "tp"),
            P(SP, None, "tp"),
            P(SP, "tp", None),
        ),
        check_vma=False,
    )
```
